512 devices in a mesh: sp: 64 (over z, y), tp: 8 (over x, core).
Axes of the slice: x: 4, y: 4, z: 16, core: 2. Of those that a mesh axis runs over, the one named last changes fastest.
Arguments:
- latent: bfloat16 [49152, 2048], P(('sp', 'tp')), may hold values from -6 to 6
- condition: float32 [2048], P('sp'), may hold values from -6 to 6
- context_condition: float32 [2048], P('sp'), may hold values from -6 to 6
- context: bfloat16 [1024, 2048], P('sp'), may hold values from -6 to 6
- norm_gain: float32 [2048], replicated, may hold values from 0.1 to 1.9
- shift_weight: bfloat16 [2048, 2048], P('sp', 'tp'), may hold values from -0.375 to 0.375
- scale_weight: bfloat16 [2048, 2048], P('sp', 'tp'), may hold values from -0.375 to 0.375
- gate_weight: bfloat16 [2048, 2048], P('sp', 'tp'), may hold values from -0.375 to 0.375
- query_weight: bfloat16 [2048, 2048], P(None, 'tp'), may hold values from -2 to 2
- key_matrix: bfloat16 [2048, 1024], P(None, 'tp'), may hold values from -2 to 2
- value_matrix: bfloat16 [2048, 1024], P(None, 'tp'), may hold values from -0.125 to 0.125
- sink_logit_head: float32 [16], P('tp'), may hold values from 6 to 10
- out_weight: bfloat16 [2048, 2048], P('tp'), may hold values from -0.125 to 0.125
Outputs:
- updated: bfloat16 [49152, 2048], P(('sp', 'tp'))
The draws below stay inside these ranges and needn't reach their ends.
All inputs are finite; a program needn't handle non-finite values.
Results may differ from the reference program's by a relative error of at most 0.012.
The reference program's roundings to bfloat16 on the way count: a program that leaves them out, or rounds other values in their place, can miss the bound.
Values may be sent and summed in bfloat16 or wider, within the bound.
A program may use at most 64 MiB of HBM per device.

```python
import jax
import jax.numpy as jnp
from jax import lax

MODEL_DIM = 2048
QUERY_HEADS = 16
KEY_VALUE_HEADS = 8
HEAD_DIM = 128
WINDOW_REACH = 128
GRID_W = 64
CTX = 1024
TOKENS = 49152
N_TP = 8


def query_shared_group(key):
    return jax.random.normal(jax.random.fold_in(key, 101), (MODEL_DIM, QUERY_HEADS * HEAD_DIM), jnp.float32) * MODEL_DIM ** (-0.5)


def draw_query_weight(key, part):
    return query_shared_group(key).astype(jnp.bfloat16)


def draw_key_matrix(key, part):
    sampled_weights = jax.random.normal(jax.random.fold_in(key, 202), (MODEL_DIM, KEY_VALUE_HEADS * HEAD_DIM), jnp.float32) * MODEL_DIM ** (-0.5)
    return sampled_weights.astype(jnp.bfloat16)


def raised(drawn, stream_key, source, target, shards_of, factor):
    owner, partner = [(jnp.arange(drawn.shape[dim]) // (drawn.shape[dim] // shards_of)).reshape([-1 if axis == dim else 1 for axis in range(drawn.ndim)]) for dim in (source, target)]
    chosen = jax.random.permutation(stream_key, shards_of)[partner]
    strong = (owner == chosen) | (owner == (partner + shards_of // 2) % shards_of)
    return jnp.where(strong, factor * drawn, drawn)


def level_of(stream_key, dims, cuts, low, top_value):
    def one(axis_at, parts):
        steps = jax.random.uniform(jax.random.fold_in(jax.random.fold_in(stream_key, 6), axis_at), (parts,), jnp.float32, low / len(cuts), top_value / len(cuts))
        return jnp.repeat(jnp.exp(steps), dims[axis_at] // parts).reshape((-1,) + (1,) * (len(dims) - axis_at - 1))

    gain = one(*cuts[0])
    for cut in cuts[1:]:
        gain = gain * one(*cut)
    return gain


def normal_values(key, dims, spread, most, cuts=(), kind=jnp.bfloat16):
    drawn = spread * jax.random.normal(key, dims, jnp.float32)
    if cuts:
        drawn = drawn * level_of(key, dims, cuts, -0.22, 0.18)
    return jnp.clip(drawn, -most, most).astype(kind)


def heavy_noise(stream_key, extent, scale, most, cuts, heavy, kind=jnp.bfloat16):
    values = scale * jax.random.normal(stream_key, extent, jnp.float32)
    if cuts:
        values = values * level_of(stream_key, extent, cuts, -0.22, 0.18)
    return jnp.clip(raised(values, jax.random.fold_in(stream_key, 3), *heavy), -most, most).astype(kind)


def setup_inputs(seed: int = 0) -> dict:
    key_list = jax.random.split(jax.random.key(seed), 14)
    latent = normal_values(key_list[0], (TOKENS, MODEL_DIM), 1.0, 6.0, ((0, 512),))
    condition = normal_values(key_list[1], (MODEL_DIM,), 1.0, 6.0, ((0, 64),), jnp.float32)
    context_condition = normal_values(key_list[2], (MODEL_DIM,), 1.0, 6.0, ((0, 64),), jnp.float32)
    context = normal_values(key_list[3], (CTX, MODEL_DIM), 1.0, 6.0, ((0, 64),))
    norm_gain = jnp.clip(1.0 + 0.18 * jax.random.normal(key_list[4], (MODEL_DIM,), jnp.float32), 0.1, 1.9)
    shift_weight = heavy_noise(key_list[5], (MODEL_DIM, MODEL_DIM), MODEL_DIM ** -0.5, 0.375, ((0, 64), (1, 8)), (0, 1, 64, 4.0))
    scale_weight = heavy_noise(key_list[6], (MODEL_DIM, MODEL_DIM), MODEL_DIM ** -0.5, 0.375, ((0, 64), (1, 8)), (0, 1, 64, 4.0))
    gate_weight = heavy_noise(key_list[7], (MODEL_DIM, MODEL_DIM), MODEL_DIM ** -0.5, 0.375, ((0, 64), (1, 8)), (0, 1, 64, 4.0))
    query_weight = draw_query_weight(jax.random.fold_in(key_list[13], 71), 0)
    key_matrix = draw_key_matrix(jax.random.fold_in(key_list[13], 71), 0)
    value_matrix = normal_values(key_list[10], (MODEL_DIM, KEY_VALUE_HEADS * HEAD_DIM), MODEL_DIM ** -0.5, 0.125, ((1, 8),))
    sink_logit_head = jnp.clip(6.0 + 4.0 * jax.random.uniform(key_list[11], (QUERY_HEADS,), jnp.float32) ** level_of(key_list[11], (QUERY_HEADS,), ((0, 8),), -0.2, 0.2), 6.0, 10.0)
    out_weight = normal_values(key_list[12], (QUERY_HEADS * HEAD_DIM, MODEL_DIM), (QUERY_HEADS * HEAD_DIM) ** -0.5, 0.125, ((0, 8),))
    return {"latent": latent, "condition": condition, "context_condition": context_condition, "context": context, "norm_gain": norm_gain, "shift_weight": shift_weight, "scale_weight": scale_weight, "gate_weight": gate_weight, "query_weight": query_weight, "key_matrix": key_matrix, "value_matrix": value_matrix, "sink_logit_head": sink_logit_head, "out_weight": out_weight}


NORM_EPS = 1e-05
MASKED_SCORE = -1e+30

def rotate(vectors, position):
    quarter = HEAD_DIM // 4
    grid_row = (position // GRID_W).astype(jnp.float32)
    grid_col = (position % GRID_W).astype(jnp.float32)
    inv_freq = 10000.0 ** (-jnp.arange(0, HEAD_DIM // 2, 2, dtype=jnp.float32) / (HEAD_DIM // 2))
    angles = jnp.concatenate([grid_row[:, None] * inv_freq, grid_col[:, None] * inv_freq], axis=-1)
    cosine_table = jnp.cos(angles).reshape(-1, 1, 2, quarter)
    sine_table = jnp.sin(angles).reshape(-1, 1, 2, quarter)
    pieces = vectors.reshape(vectors.shape[0], vectors.shape[1], 2, 2, quarter)
    first_half = pieces[..., 0, :]
    second_half = pieces[..., 1, :]
    turned = jnp.stack([first_half * cosine_table - second_half * sine_table, first_half * sine_table + second_half * cosine_table], axis=-2)
    return turned.reshape(vectors.shape)

def modulation(vector, weight):
    active = jax.nn.silu(vector).astype(jnp.bfloat16)
    return jnp.dot(active[None, :], weight, preferred_element_type=jnp.float32)[0]

def modulated_norm(rows_in, norm_gain, shift, scale):
    floats = rows_in.astype(jnp.float32)
    normed = floats * lax.rsqrt(lax.optimization_barrier(jnp.mean(floats * floats, axis=-1, keepdims=True)) + NORM_EPS) * norm_gain
    return (normed * (1.0 + scale) + shift).astype(jnp.bfloat16)

def attend(queries, joined_keys, joined_values, context_key_rows, context_value_rows, sink_logit_head):
    latent_token_count = queries.shape[0]
    blocks = latent_token_count // WINDOW_REACH
    queries_per_group = QUERY_HEADS // KEY_VALUE_HEADS
    padding = ((WINDOW_REACH, WINDOW_REACH), (0, 0), (0, 0))
    keys_pad = jnp.pad(joined_keys, padding)
    values_pad = jnp.pad(joined_values, padding)
    ctx_key_f = context_key_rows.astype(jnp.float32)
    ctx_value_f = context_value_rows.astype(jnp.float32)
    factor = HEAD_DIM ** (-0.5)
    sink_logit_rows = sink_logit_head.reshape(KEY_VALUE_HEADS, queries_per_group, 1, 1)

    def one_block(block_index):
        begin_row = block_index * WINDOW_REACH
        query_row_block = lax.dynamic_slice_in_dim(queries, begin_row, WINDOW_REACH, 0)
        query_row_block = query_row_block.reshape(WINDOW_REACH, KEY_VALUE_HEADS, queries_per_group, HEAD_DIM).astype(jnp.float32)
        band_keys = lax.dynamic_slice_in_dim(keys_pad, begin_row, 3 * WINDOW_REACH, 0).astype(jnp.float32)
        band_values = lax.dynamic_slice_in_dim(values_pad, begin_row, 3 * WINDOW_REACH, 0).astype(jnp.float32)
        band_scores = jnp.einsum('qhgd,khd->hgqk', query_row_block, band_keys) * factor
        query_pos = begin_row + jnp.arange(WINDOW_REACH, dtype=jnp.int32)[:, None]
        key_pos = begin_row - WINDOW_REACH + jnp.arange(3 * WINDOW_REACH, dtype=jnp.int32)[None, :]
        allowed = (jnp.abs(key_pos - query_pos) <= WINDOW_REACH) & (key_pos >= 0) & (key_pos < latent_token_count)
        band_scores = jnp.where(allowed[None, None], band_scores, MASKED_SCORE)
        ctx_scores = jnp.einsum('qhgd,chd->hgqc', query_row_block, ctx_key_f) * factor
        maxima = jnp.maximum(jnp.maximum(lax.optimization_barrier(jnp.max(band_scores, axis=-1, keepdims=True)), lax.optimization_barrier(jnp.max(ctx_scores, axis=-1, keepdims=True))), sink_logit_rows)
        band_exp = jnp.exp(band_scores - maxima)
        ctx_exp = jnp.exp(ctx_scores - maxima)
        denominator = lax.optimization_barrier(jnp.sum(band_exp, axis=-1, keepdims=True)) + lax.optimization_barrier(jnp.sum(ctx_exp, axis=-1, keepdims=True)) + jnp.exp(sink_logit_rows - maxima)
        band_weights = (band_exp / denominator).astype(jnp.bfloat16).astype(jnp.float32)
        ctx_weights = (ctx_exp / denominator).astype(jnp.bfloat16).astype(jnp.float32)
        summed = jnp.einsum('hgqk,khd->qhgd', band_weights, band_values) + jnp.einsum('hgqc,chd->qhgd', ctx_weights, ctx_value_f)
        return summed.astype(jnp.bfloat16).reshape(WINDOW_REACH, QUERY_HEADS * HEAD_DIM)
    blocks_out = lax.map(one_block, jnp.arange(blocks, dtype=jnp.int32))
    return blocks_out.reshape(latent_token_count, QUERY_HEADS * HEAD_DIM)

def reference(latent, condition, context_condition, context, norm_gain, shift_weight, scale_weight, gate_weight, query_weight, key_matrix, value_matrix, sink_logit_head, out_weight):
    shift = modulation(condition, shift_weight)
    scale = modulation(condition, scale_weight)
    gate = modulation(condition, gate_weight)
    ctx_shift = modulation(context_condition, shift_weight)
    ctx_scale = modulation(context_condition, scale_weight)
    hidden_state = modulated_norm(latent, norm_gain, shift, scale)
    ctx_hidden = modulated_norm(context, norm_gain, ctx_shift, ctx_scale)
    latent_token_count = latent.shape[0]
    position = jnp.arange(latent_token_count, dtype=jnp.int32)
    queries = jnp.dot(hidden_state, query_weight, preferred_element_type=jnp.float32).reshape(latent_token_count, QUERY_HEADS, HEAD_DIM)
    queries = rotate(queries, position).astype(jnp.bfloat16)
    joined_keys = jnp.dot(hidden_state, key_matrix, preferred_element_type=jnp.float32).reshape(latent_token_count, KEY_VALUE_HEADS, HEAD_DIM)
    joined_keys = rotate(joined_keys, position).astype(jnp.bfloat16)
    joined_values = jnp.dot(hidden_state, value_matrix, preferred_element_type=jnp.float32).astype(jnp.bfloat16)
    joined_values = joined_values.reshape(latent_token_count, KEY_VALUE_HEADS, HEAD_DIM)
    context_key_rows = jnp.dot(ctx_hidden, key_matrix, preferred_element_type=jnp.float32).astype(jnp.bfloat16)
    context_value_rows = jnp.dot(ctx_hidden, value_matrix, preferred_element_type=jnp.float32).astype(jnp.bfloat16)
    context_key_rows = context_key_rows.reshape(-1, KEY_VALUE_HEADS, HEAD_DIM)
    context_value_rows = context_value_rows.reshape(-1, KEY_VALUE_HEADS, HEAD_DIM)
    attended = attend(queries, joined_keys, joined_values, context_key_rows, context_value_rows, sink_logit_head)
    group_width = QUERY_HEADS * HEAD_DIM // N_TP
    mixed_sum = jnp.zeros((latent_token_count, latent.shape[1]), jnp.float32)
    for member in range(N_TP):
        partial_value = jnp.dot(attended[:, member * group_width:(member + 1) * group_width], out_weight[member * group_width:(member + 1) * group_width], preferred_element_type=jnp.float32)
        rounded = lax.optimization_barrier(partial_value.astype(jnp.bfloat16))
        mixed_sum = mixed_sum + rounded.astype(jnp.float32)
    return (latent.astype(jnp.float32) + gate * mixed_sum).astype(jnp.bfloat16)
```

```python
import functools

import jax
import jax.numpy as jnp
from jax import lax
from jax.experimental import pallas as pl
from jax.experimental.pallas import tpu as pltpu
from jax.sharding import Mesh
from jax.sharding import PartitionSpec as P

QUERY_HEADS = 16
KEY_VALUE_HEADS = 8
HEAD_DIM = 128
WINDOW_REACH = 128
GRID_W = 64
SP = ("z", "y")
TP = ("x", "c")
ALL = ("z", "y", "x", "c")
MESH = pl.DeviceIdType.MESH

NORM_EPS = 1e-05
MASKED_SCORE = -1e30
NZ, NY, NX, NC = 16, 4, 4, 2
F32 = jnp.float32
BF16 = jnp.bfloat16


def wrap(value, size):
    return lax.rem(value + size, size)


def remote(src, dst, send, recv, device):
    return pltpu.make_async_remote_copy(
        src_ref=src,
        dst_ref=dst,
        send_sem=send,
        recv_sem=recv,
        device_id=device,
        device_id_type=MESH,
    )


def greet(peers):
    barrier = pltpu.get_barrier_semaphore()
    for peer in peers:
        pl.semaphore_signal(barrier, inc=1, device_id=peer, device_id_type=MESH)
    return lambda: pl.semaphore_wait(barrier, len(peers))


def norm_rows(rows, gain, shift, scale):
    floats = rows.astype(F32)
    mean = jnp.mean(floats * floats, axis=-1, keepdims=True)
    normed = floats * lax.rsqrt(mean + NORM_EPS) * gain
    return (normed * (1.0 + scale) + shift).astype(BF16)


def gather_kernel(
    lat_ref, ctx_ref, gain_ref, cond_ref, cctx_ref, shift_ref, scale_ref, gate_ref,
    hid_ref, ctxh_ref, mod_ref,
    rows, parts, ybuf, zsrc, zbuf, gsrc, gbuf,
    y_send, y_recv, z_send, z_recv, g_send, g_recv, a_send, a_recv, p_send, p_recv,
):
    z, y, x, c = (lax.axis_index(a) for a in ALL)
    tp = x * NC + c
    right, left = wrap(x + 1, NX), wrap(x - 1, NX)
    opposite = wrap(x + 2, NX)
    plane = [
        (dy, dx, dc)
        for dy in range(NY)
        for dx in range(NX)
        for dc in range(NC)
        if (dy, dx, dc) != (0, 0, 0)
    ]

    def plane_peer(dy, dx, dc):
        return {"y": wrap(y + dy, NY), "x": wrap(x + dx, NX), "c": wrap(c + dc, NC)}

    entered = greet(
        [plane_peer(*p) for p in plane] + [{"z": wrap(z + d, NZ)} for d in range(1, NZ)]
    )

    row = lax.broadcasted_iota(jnp.int32, (8, 32), 0)
    vectors = jnp.where(
        row == 0,
        jnp.broadcast_to(cond_ref[...], (8, 32)),
        jnp.broadcast_to(cctx_ref[...], (8, 32)),
    )
    active = (vectors / (1.0 + jnp.exp(-vectors))).astype(BF16)
    shift_part = jnp.dot(active, shift_ref[...], preferred_element_type=F32)
    scale_part = jnp.dot(active, scale_ref[...], preferred_element_type=F32)
    gate_part = jnp.dot(active, gate_ref[...], preferred_element_type=F32)
    for t in range(2):
        cols = slice(t * 128, t * 128 + 128)
        parts[t] = jnp.concatenate(
            [shift_part[0:1, cols], scale_part[0:1, cols], gate_part[0:1, cols], gate_part[0:1, cols]],
            axis=0,
        )
        parts[2 + t] = jnp.concatenate(
            [shift_part[1:2, cols], scale_part[1:2, cols], scale_part[1:2, cols], scale_part[1:2, cols]],
            axis=0,
        )
    rows[tp] = lat_ref[...]

    entered()

    half = (pl.ds(0, 48), pl.ds(48, 48))
    partner = {"c": 1 - c}
    y_copies = []
    for d in range(1, NY):
        target = wrap(y + d, NY)
        copy = remote(parts.at[target], ybuf.at[d], y_send.at[d], y_recv.at[d], {"y": target})
        copy.start()
        y_copies.append(copy)
    sent = []

    def send_half(owner, h, to, k):
        source = lat_ref.at[half[h]] if owner is None else rows.at[owner, half[h]]
        slot = rows.at[tp if owner is None else owner, half[h]]
        copy = remote(source, slot, a_send.at[k], a_recv.at[k], {"x": to})
        copy.start()
        sent.append(copy)

    def send_partner(owner, h, k):
        if owner is None:
            copy = remote(lat_ref, rows.at[tp], p_send.at[k], p_recv.at[k], partner)
        else:
            copy = remote(
                rows.at[owner, half[h]], rows.at[owner, half[h]], p_send.at[k], p_recv.at[k], partner
            )
        copy.start()
        sent.append(copy)

    from_left, from_right = left * NC + c, right * NC + c
    from_opposite = opposite * NC + c

    def arrived(owner, h, k):
        slot = rows.at[owner, half[h]]
        remote(slot, slot, a_send.at[k], a_recv.at[k], {"x": right}).wait_recv()

    send_half(None, 0, right, 0)
    send_half(None, 1, left, 1)
    send_half(None, 1, right, 2)
    send_half(None, 0, left, 3)
    send_partner(None, 0, 0)

    for copy in y_copies:
        copy.wait_recv()
    zsrc[...] = parts[y] + ybuf[1] + ybuf[2] + ybuf[3]

    arrived(from_left, 0, 0)
    send_half(from_left, 0, right, 4)
    send_partner(from_left, 0, 1)
    z_copies = []
    for d in range(1, NZ):
        copy = remote(zsrc, zbuf.at[d], z_send.at[d], z_recv.at[d], {"z": wrap(z + d, NZ)})
        copy.start()
        z_copies.append(copy)
    arrived(from_right, 1, 1)
    send_half(from_right, 1, left, 5)
    send_partner(from_right, 1, 2)

    for copy in z_copies:
        copy.wait_recv()
    total = zsrc[...]
    for d in range(1, NZ):
        total = total + zbuf[d]
    gsrc[...] = total
    gbuf[tp, y] = total
    arrived(from_left, 1, 2)
    send_partner(from_left, 1, 3)
    arrived(from_right, 0, 3)
    send_partner(from_right, 0, 4)
    g_copies = []
    for k, p in enumerate(plane):
        copy = remote(gsrc, gbuf.at[tp, y], g_send.at[k], g_recv.at[k], plane_peer(*p))
        copy.start()
        g_copies.append(copy)
    arrived(from_opposite, 0, 4)
    send_partner(from_opposite, 0, 5)
    arrived(from_opposite, 1, 5)
    send_partner(from_opposite, 1, 6)
    for copy in g_copies:
        copy.wait_recv()
    for owner in range(NX * NC):
        for t in range(2):
            cols = pl.ds((owner * 2 + t) * 128, 128)
            mod_ref[0:4, cols] = gbuf[owner, t]
            mod_ref[4:8, cols] = gbuf[owner, 2 + t]
    ctxh_ref[...] = norm_rows(ctx_ref[...], gain_ref[...], mod_ref[4:5, :], mod_ref[5:6, :])
    mate = x * NC + 1 - c
    remote(lat_ref, rows.at[mate], p_send.at[0], p_recv.at[0], partner).wait_recv()
    others = [(left, 0, 1), (right, 1, 2), (left, 1, 3), (right, 0, 4), (opposite, 0, 5), (opposite, 1, 6)]
    for chip, h, k in others:
        slot = rows.at[chip * NC + 1 - c, half[h]]
        remote(slot, slot, p_send.at[k], p_recv.at[k], partner).wait_recv()

    gain = gain_ref[...]
    shift = mod_ref[0:1, :]
    scale = mod_ref[1:2, :]

    def one(i, carry):
        owner = i // 6
        part = pl.ds(pl.multiple_of((i % 6) * 16, 16), 16)
        hid_ref[owner, part] = norm_rows(rows[owner, part], gain, shift, scale)
        return carry

    lax.fori_loop(0, NX * NC * 6, one, 0)
    for copy in sent + y_copies + z_copies + g_copies:
        copy.wait_send()


def gathered(latent, context, norm_gain, condition, context_condition, shift_w, scale_w, gate_w):
    rows, width = latent.shape
    vmem = pl.BlockSpec(memory_space=pltpu.VMEM)
    tps = NX * NC
    return pl.pallas_call(
        gather_kernel,
        out_shape=(
            jax.ShapeDtypeStruct((tps, rows, width), BF16),
            jax.ShapeDtypeStruct(context.shape, BF16),
            jax.ShapeDtypeStruct((8, width), F32),
        ),
        in_specs=[vmem] * 8,
        out_specs=(vmem,) * 3,
        scratch_shapes=[
            pltpu.VMEM((tps, rows, width), BF16),
            pltpu.VMEM((4, 4, 128), F32),
            pltpu.VMEM((NY, 4, 128), F32),
            pltpu.VMEM((4, 128), F32),
            pltpu.VMEM((NZ, 4, 128), F32),
            pltpu.VMEM((4, 128), F32),
            pltpu.VMEM((tps, NY, 4, 128), F32),
            pltpu.SemaphoreType.DMA((NY,)),
            pltpu.SemaphoreType.DMA((NY,)),
            pltpu.SemaphoreType.DMA((NZ,)),
            pltpu.SemaphoreType.DMA((NZ,)),
            pltpu.SemaphoreType.DMA((31,)),
            pltpu.SemaphoreType.DMA((31,)),
            pltpu.SemaphoreType.DMA((6,)),
            pltpu.SemaphoreType.DMA((6,)),
            pltpu.SemaphoreType.DMA((7,)),
            pltpu.SemaphoreType.DMA((7,)),
        ],
        compiler_params=pltpu.CompilerParams(
            collective_id=0, has_side_effects=True, vmem_limit_bytes=40 * 1024 * 1024
        ),
        cost_estimate=pl.CostEstimate(flops=10**9, bytes_accessed=10**7, transcendentals=0),
        name="gather",
    )(
        latent, context, norm_gain.reshape(1, -1), condition.reshape(1, -1),
        context_condition.reshape(1, -1), shift_w, scale_w, gate_w,
    )


def output_kernel(
    att_ref, wo_ref, lat_ref, mod_ref, out_ref,
    wo_mate, att_mate, opp_src, right_src, left_src, opp_left, opp_right, from_left, from_right,
    m_send, m_recv, s_send, s_recv,
):
    x, c = lax.axis_index("x"), lax.axis_index("c")
    right, left = wrap(x + 1, NX), wrap(x - 1, NX)
    entered = greet([{"x": right}, {"x": left}, {"c": 1 - c}])
    entered()
    partner = {"c": 1 - c}
    mates = [remote(wo_ref, wo_mate, m_send.at[4], m_recv.at[4], partner)]
    for chip in range(NX):
        mates.append(
            remote(att_ref.at[chip * NC + 1 - c], att_mate.at[chip], m_send.at[chip], m_recv.at[chip], partner)
        )
    for copy in mates:
        copy.start()
    for copy in mates:
        copy.wait_recv()

    def product(chip, h):
        cols = slice(h * 1024, h * 1024 + 1024)
        return jnp.dot(
            att_ref[chip * NC + c], wo_ref[:, cols], preferred_element_type=F32
        ) + jnp.dot(att_mate[chip], wo_mate[:, cols], preferred_element_type=F32)

    sent = []

    def send(src, dst, k, to):
        copy = remote(src, dst, s_send.at[k], s_recv.at[k], {"x": to})
        copy.start()
        sent.append(copy)
        return copy

    across = wrap(x + 2, NX)
    opp_src[0] = product(across, 0).astype(BF16)
    first_left = send(opp_src.at[0], opp_left, 0, right)
    opp_src[1] = product(across, 1).astype(BF16)
    first_right = send(opp_src.at[1], opp_right, 1, left)
    right_src[1] = product(right, 1).astype(BF16)
    a = send(right_src.at[1], from_left.at[1], 2, right)
    left_src[0] = product(left, 0).astype(BF16)
    b = send(left_src.at[0], from_right.at[0], 3, left)
    right_part = product(right, 0)
    first_left.wait_recv()
    right_src[0] = (right_part + opp_left[...].astype(F32)).astype(BF16)
    d = send(right_src.at[0], from_left.at[0], 4, right)
    left_part = product(left, 1)
    first_right.wait_recv()
    left_src[1] = (left_part + opp_right[...].astype(F32)).astype(BF16)
    e = send(left_src.at[1], from_right.at[1], 5, left)
    a.wait_recv()
    b.wait_recv()
    d.wait_recv()
    e.wait_recv()
    for h in range(2):
        cols = slice(h * 1024, h * 1024 + 1024)
        total = product(x, h) + from_left[h].astype(F32) + from_right[h].astype(F32)
        out_ref[:, cols] = (
            lat_ref[:, cols].astype(F32) + mod_ref[2:3, cols] * total
        ).astype(BF16)
    for copy in mates + sent:
        copy.wait_send()


def projected_out(attended, out_weight, latent, mod):
    rows, width = latent.shape
    vmem = pl.BlockSpec(memory_space=pltpu.VMEM)
    tps = NX * NC
    half = width // 2
    return pl.pallas_call(
        output_kernel,
        out_shape=jax.ShapeDtypeStruct((rows, width), BF16),
        in_specs=[vmem] * 4,
        out_specs=vmem,
        scratch_shapes=[
            pltpu.VMEM(out_weight.shape, BF16),
            pltpu.VMEM((NX, rows, attended.shape[1]), BF16),
            pltpu.VMEM((2, rows, half), BF16),
            pltpu.VMEM((2, rows, half), BF16),
            pltpu.VMEM((2, rows, half), BF16),
            pltpu.VMEM((rows, half), BF16),
            pltpu.VMEM((rows, half), BF16),
            pltpu.VMEM((2, rows, half), BF16),
            pltpu.VMEM((2, rows, half), BF16),
            pltpu.SemaphoreType.DMA((5,)),
            pltpu.SemaphoreType.DMA((5,)),
            pltpu.SemaphoreType.DMA((6,)),
            pltpu.SemaphoreType.DMA((6,)),
        ],
        compiler_params=pltpu.CompilerParams(
            collective_id=1, has_side_effects=True, vmem_limit_bytes=40 * 1024 * 1024
        ),
        cost_estimate=pl.CostEstimate(flops=10**9, bytes_accessed=10**7, transcendentals=0),
        name="output",
    )(attended.reshape(tps, rows, -1), out_weight, latent, mod)


def padded_2(block, sides, width):
    for axis, dim in sides:
        count = lax.axis_size(axis)
        forward = [(i, i + 1) for i in range(count - 1)]
        backward = [(target, source) for source, target in forward]
        low = lax.ppermute(
            lax.slice_in_dim(block, block.shape[dim] - width, None, axis=dim), axis, forward
        )
        high = lax.ppermute(lax.slice_in_dim(block, 0, width, axis=dim), axis, backward)
        block = jnp.concatenate([low, block, high], axis=dim)
    return block


def sent_to_all(x, axis):
    peers = lax.axis_size(axis)
    return lax.all_to_all(jnp.broadcast_to(x[None], (peers, *x.shape)), axis, 0, 0, tiled=True)


def laid_out(blocks, dim):
    blocks = jnp.moveaxis(blocks, 0, dim)
    shape = blocks.shape
    return blocks.reshape(*shape[:dim], shape[dim] * shape[dim + 1], *shape[dim + 2 :])


def gathered_copies(x, axis, dim):
    blocks = sent_to_all(x, axis)
    return laid_out(blocks, dim)


def rotate(vectors, position):
    quarter = HEAD_DIM // 4
    grid_row = (position // GRID_W).astype(jnp.float32)
    grid_col = (position % GRID_W).astype(jnp.float32)
    inv_freq = 10000.0 ** (-jnp.arange(0, HEAD_DIM // 2, 2, dtype=jnp.float32) / (HEAD_DIM // 2))
    angles = jnp.concatenate([grid_row[:, None] * inv_freq, grid_col[:, None] * inv_freq], axis=-1)
    cosine_table = jnp.cos(angles).reshape(-1, 1, 2, quarter)
    sine_table = jnp.sin(angles).reshape(-1, 1, 2, quarter)
    pieces = vectors.reshape(vectors.shape[0], vectors.shape[1], 2, 2, quarter)
    first_half = pieces[..., 0, :]
    second_half = pieces[..., 1, :]
    turned = jnp.stack(
        [
            first_half * cosine_table - second_half * sine_table,
            first_half * sine_table + second_half * cosine_table,
        ],
        axis=-2,
    )
    return turned.reshape(vectors.shape)


def shards(
    latent,
    condition,
    context_condition,
    context,
    norm_gain,
    shift_weight,
    scale_weight,
    gate_weight,
    query_weight,
    key_matrix,
    value_matrix,
    sink_logit_head,
    out_weight,
):
    tp_count = NX * NC
    group_rows = latent.shape[0] * tp_count
    offset = lax.axis_index(SP) * group_rows
    total_rows = group_rows * lax.axis_size(SP)
    hidden, ctx_hidden, mod = gathered(
        latent, context, norm_gain, condition, context_condition,
        shift_weight, scale_weight, gate_weight,
    )
    query_width = query_weight.shape[1]
    pair_width = key_matrix.shape[1]
    block_rows = hidden.reshape(group_rows, -1)
    row_count = block_rows.shape[0]
    position = offset + jnp.arange(row_count, dtype=jnp.int32)
    query_row_block = jnp.dot(block_rows, query_weight, preferred_element_type=jnp.float32)
    query_row_block = rotate(query_row_block.reshape(row_count, -1, HEAD_DIM), position)
    key_rows = jnp.dot(block_rows, key_matrix, preferred_element_type=jnp.float32)
    key_rows = rotate(key_rows.reshape(row_count, -1, HEAD_DIM), position)
    value_rows = jnp.dot(block_rows, value_matrix, preferred_element_type=jnp.float32)
    projected = jnp.concatenate(
        [
            query_row_block.reshape(row_count, query_width),
            key_rows.reshape(row_count, pair_width),
            value_rows,
        ],
        axis=1,
    ).astype(jnp.bfloat16)
    padded = padded_2(projected[:, query_width:], ((SP, 0),), WINDOW_REACH)
    ctx_pairs = gathered_copies(
        jnp.concatenate(
            [
                jnp.dot(ctx_hidden, key_matrix, preferred_element_type=jnp.float32),
                jnp.dot(ctx_hidden, value_matrix, preferred_element_type=jnp.float32),
            ],
            axis=1,
        ).astype(jnp.bfloat16),
        SP,
        0,
    )
    blocks = group_rows // WINDOW_REACH
    kv_local = pair_width // HEAD_DIM
    queries_per_group = QUERY_HEADS // KEY_VALUE_HEADS
    query_blocks = projected[:, :query_width].reshape(
        blocks, WINDOW_REACH, kv_local, queries_per_group, HEAD_DIM
    )
    key_pad = padded[:, :pair_width].reshape(blocks + 2, WINDOW_REACH, kv_local, HEAD_DIM)
    value_pad = padded[:, pair_width:].reshape(blocks + 2, WINDOW_REACH, kv_local, HEAD_DIM)
    band_keys = jnp.concatenate([key_pad[:-2], key_pad[1:-1], key_pad[2:]], axis=1)
    band_values = jnp.concatenate([value_pad[:-2], value_pad[1:-1], value_pad[2:]], axis=1)
    context_key_rows = ctx_pairs[:, :pair_width].reshape(-1, kv_local, HEAD_DIM)
    context_value_rows = ctx_pairs[:, pair_width:].reshape(-1, kv_local, HEAD_DIM)
    factor = HEAD_DIM ** (-0.5)
    band_scores = (
        jnp.einsum("nqhgd,nkhd->nhgqk", query_blocks, band_keys, preferred_element_type=jnp.float32)
        * factor
    )
    block_ids = jnp.arange(blocks, dtype=jnp.int32)[:, None, None]
    query_pos = (
        offset + block_ids * WINDOW_REACH + jnp.arange(WINDOW_REACH, dtype=jnp.int32)[None, :, None]
    )
    key_pos = (
        offset
        + (block_ids - 1) * WINDOW_REACH
        + jnp.arange(3 * WINDOW_REACH, dtype=jnp.int32)[None, None, :]
    )
    allowed = (
        (jnp.abs(key_pos - query_pos) <= WINDOW_REACH) & (key_pos >= 0) & (key_pos < total_rows)
    )
    band_scores = jnp.where(allowed[:, None, None], band_scores, MASKED_SCORE)
    ctx_scores = (
        jnp.einsum(
            "nqhgd,chd->nhgqc", query_blocks, context_key_rows, preferred_element_type=jnp.float32
        )
        * factor
    )
    sink_logit_rows = sink_logit_head.reshape(1, kv_local, queries_per_group, 1, 1)
    maxima = jnp.maximum(
        jnp.maximum(
            jnp.max(band_scores, axis=-1, keepdims=True),
            jnp.max(ctx_scores, axis=-1, keepdims=True),
        ),
        sink_logit_rows,
    )
    band_exp = jnp.exp(band_scores - maxima)
    ctx_exp = jnp.exp(ctx_scores - maxima)
    denominator = (
        jnp.sum(band_exp, axis=-1, keepdims=True)
        + jnp.sum(ctx_exp, axis=-1, keepdims=True)
        + jnp.exp(sink_logit_rows - maxima)
    )
    band_weights = (band_exp / denominator).astype(jnp.bfloat16)
    ctx_weights = (ctx_exp / denominator).astype(jnp.bfloat16)
    attended = jnp.einsum(
        "nhgqk,nkhd->nqhgd", band_weights, band_values, preferred_element_type=jnp.float32
    ) + jnp.einsum(
        "nhgqc,chd->nqhgd", ctx_weights, context_value_rows, preferred_element_type=jnp.float32
    )
    attended = attended.astype(jnp.bfloat16).reshape(group_rows, query_width)
    return projected_out(attended, out_weight, latent, mod)


def solution(mesh):
    torus = Mesh(mesh.devices.reshape(NZ, NY, NX, NC), ALL)
    return jax.shard_map(
        shards,
        mesh=torus,
        in_specs=(
            P(ALL, None),
            P(SP),
            P(SP),
            P(SP, None),
            P(),
            P(SP, TP),
            P(SP, TP),
            P(SP, TP),
            P(None, TP),
            P(None, TP),
            P(None, TP),
            P(TP),
            P(TP, None),
        ),
        out_specs=P(ALL, None),
        check_vma=False,
    )
```

```python
import functools

import jax
import jax.numpy as jnp
import numpy as np
from jax import lax
from jax.experimental import pallas as pl
from jax.experimental.pallas import tpu as pltpu
from jax.sharding import Mesh
from jax.sharding import PartitionSpec as P

HEAD_DIM = 128
WINDOW_REACH = 128
GRID_W = 64
SP = ("z", "y")
TP = ("x", "c")
ALL = ("z", "y", "x", "c")
MESH = pl.DeviceIdType.MESH

NORM_EPS = 1e-05
MASKED_SCORE = -1e30
LOG2E = 1.4426950408889634
NZ, NY, NX, NC = 16, 4, 4, 2
NTP = NX * NC
WIDTH = 2048
ROWS = 96
GROUP = ROWS * NTP
CHIP = ROWS * NC
CTX_ROWS = 16
WIN = 512
F32 = jnp.float32
BF16 = jnp.bfloat16
PLANE = [
    (dy, dx, dc)
    for dy in range(NY)
    for dx in range(NX)
    for dc in range(NC)
    if (dy, dx, dc) != (0, 0, 0)
]


def wrap(value, size):
    return lax.rem(value + size, size)


def remote(src, dst, send, recv, device):
    return pltpu.make_async_remote_copy(
        src_ref=src,
        dst_ref=dst,
        send_sem=send,
        recv_sem=recv,
        device_id=device,
        device_id_type=MESH,
    )


def rows_at(start, count):
    return pl.ds(pl.multiple_of(start, 16), count)


def block_kernel(
    lat_hbm, ctx_hbm, gain_hbm, cond_hbm, cctx_hbm, sw_hbm, cw_hbm, gw_hbm,
    wq_hbm, wk_hbm, wv_hbm, sink_hbm, wo_hbm, freq_hbm,
    out_ref,
    lat, ctx, gain, cond, cctx, sw, cw, gw, wqkv, sink, wo, freq,
    rows, parts, ybuf, zsrc, zbuf, gsrc, gbuf, mod, amp, camp,
    cos_t, sin_t, band, hid, qkv, q, kv, ctxkv,
    att, att_mate, wo_mate, opp_src, right_src, left_src, opp_left, opp_right, from_left, from_right,
    l_sem, y_send, y_recv, z_send, z_recv, g_send, g_recv, a_send, a_recv, p_send, p_recv,
    c_send, c_recv, d_send, d_recv, h_send, h_recv, m_send, m_recv, s_send, s_recv,
):
    z, y, x, c = (lax.axis_index(a) for a in ALL)
    tp = x * NC + c
    sp = z * NY + y
    right, left, across = wrap(x + 1, NX), wrap(x - 1, NX), wrap(x + 2, NX)
    up, down = wrap(y + 1, NY), wrap(y - 1, NY)
    partner = {"c": 1 - c}
    after = {"z": wrap(z + (y + 1) // NY, NZ), "y": up}
    before = {"z": wrap(z - (NY - y) // NY, NZ), "y": down}

    def plane_peer(dy, dx, dc):
        return {"y": wrap(y + dy, NY), "x": wrap(x + dx, NX), "c": wrap(c + dc, NC)}

    barrier = pltpu.get_barrier_semaphore()
    peers = [{"z": wrap(z + d, NZ)} for d in range(1, NZ)]
    peers += [plane_peer(*p) for p in PLANE] + [after, before]
    for peer in peers:
        pl.semaphore_signal(barrier, inc=1, device_id=peer, device_id_type=MESH)
    pairs = [
        (cond_hbm, cond), (cctx_hbm, cctx), (sw_hbm, sw), (cw_hbm, cw), (gw_hbm, gw),
        (lat_hbm, lat), (freq_hbm, freq), (ctx_hbm, ctx), (gain_hbm, gain), (sink_hbm, sink),
        (wq_hbm, wqkv.at[:, pl.ds(0, 256)]), (wk_hbm, wqkv.at[:, pl.ds(256, 128)]),
        (wv_hbm, wqkv.at[:, pl.ds(384, 128)]), (wo_hbm, wo),
        (lat_hbm, rows.at[rows_at(tp * ROWS, ROWS)]),
    ]
    local = [pltpu.make_async_copy(s, d, l_sem.at[k]) for k, (s, d) in enumerate(pairs)]
    for copy in local:
        copy.start()

    for copy in local[:5]:
        copy.wait()
    row = lax.broadcasted_iota(jnp.int32, (8, 32), 0)
    vectors = jnp.where(
        row == 0, jnp.broadcast_to(cond[...], (8, 32)), jnp.broadcast_to(cctx[...], (8, 32))
    )
    active = (vectors / (1.0 + jnp.exp(-vectors))).astype(BF16)
    shift_part = jnp.dot(active, sw[...], preferred_element_type=F32)
    scale_part = jnp.dot(active, cw[...], preferred_element_type=F32)
    gate_part = jnp.dot(active, gw[...], preferred_element_type=F32)
    for t in range(2):
        cols = slice(t * 128, t * 128 + 128)
        parts[t] = jnp.concatenate(
            [shift_part[0:1, cols], scale_part[0:1, cols], gate_part[0:1, cols], gate_part[0:1, cols]],
            axis=0,
        )
        parts[2 + t] = jnp.concatenate(
            [shift_part[1:2, cols], scale_part[1:2, cols], scale_part[1:2, cols], scale_part[1:2, cols]],
            axis=0,
        )
    for copy in local[5:]:
        copy.wait()
    pl.semaphore_wait(barrier, len(peers))

    sent = []

    def send(src, dst, s_sem, r_sem, k, to):
        copy = remote(src, dst, s_sem.at[k], r_sem.at[k], to)
        copy.start()
        sent.append(copy)
        return copy

    y_copies = [
        send(parts.at[wrap(y + d, NY)], ybuf.at[d], y_send, y_recv, d, {"y": wrap(y + d, NY)})
        for d in range(1, NY)
    ]

    def piece(chip, core, h):
        return rows.at[rows_at((chip * NC + core) * ROWS + h * 48, 48)]

    def along(chip, h, k, to):
        source = lat.at[pl.ds(h * 48, 48)] if chip is None else piece(chip, c, h)
        slot = piece(x if chip is None else chip, c, h)
        send(source, slot, a_send, a_recv, k, {"x": to})

    def across_chip(chip, h, k):
        send(piece(chip, c, h), piece(chip, c, h), p_send, p_recv, k, partner)

    def arrived(chip, h, k):
        slot = piece(chip, c, h)
        remote(slot, slot, a_send.at[k], a_recv.at[k], {"x": right}).wait_recv()

    along(None, 0, 0, right)
    along(None, 1, 1, left)
    along(None, 1, 2, right)
    along(None, 0, 3, left)
    own_slot = rows.at[rows_at(tp * ROWS, ROWS)]
    send(lat, own_slot, p_send, p_recv, 0, partner)
    send(wo, wo_mate, m_send, m_recv, 4, partner)

    for copy in y_copies:
        copy.wait_recv()
    zsrc[...] = parts[y] + ybuf[1] + ybuf[2] + ybuf[3]

    lane = lax.broadcasted_iota(jnp.int32, (64, 128), 1)
    sign = jnp.where(lane % 64 < 32, -1.0, 1.0)
    col_angle = lax.broadcasted_iota(jnp.int32, (64, 128), 0).astype(F32) * freq[...]
    col_cos, col_sin = jnp.cos(col_angle), jnp.sin(col_angle) * sign
    row_ids = sp * (GROUP // GRID_W) + lax.broadcasted_iota(jnp.int32, (16, 128), 0)
    row_angle = row_ids.astype(F32) * freq[...]
    row_cos, row_sin = jnp.cos(row_angle), jnp.sin(row_angle) * sign[0:16]

    z_copies = [
        send(zsrc, zbuf.at[d], z_send, z_recv, d, {"z": wrap(z + d, NZ)})
        for d in (8, 7, 9, 6, 10, 5, 11, 4, 12, 3, 13, 2, 14, 1, 15)
    ]
    for i in range(GROUP // GRID_W):
        block = slice(i * GRID_W, i * GRID_W + GRID_W)
        cos_t[block] = jnp.where(lane < 64, jnp.broadcast_to(row_cos[i : i + 1], (64, 128)), col_cos)
        sin_t[block] = jnp.where(lane < 64, jnp.broadcast_to(row_sin[i : i + 1], (64, 128)), col_sin)
    gap = lax.broadcasted_iota(jnp.int32, (CHIP, WIN), 1) - lax.broadcasted_iota(
        jnp.int32, (CHIP, WIN), 0
    )
    band[...] = jnp.where((gap >= 0) & (gap <= 2 * WINDOW_REACH), 0.0, MASKED_SCORE)
    kv[1024:, :] = jnp.zeros((64, 256), BF16)

    arrived(left, 0, 0)
    along(left, 0, 4, right)
    across_chip(left, 0, 1)
    arrived(right, 1, 1)
    along(right, 1, 5, left)
    across_chip(right, 1, 2)

    for copy in z_copies:
        copy.wait_recv()
    total = zsrc[...]
    for d in range(1, NZ):
        total = total + zbuf[d]
    gsrc[...] = total
    gbuf[tp, y] = total
    g_copies = [
        send(gsrc, gbuf.at[tp, y], g_send, g_recv, k, plane_peer(*p)) for k, p in enumerate(PLANE)
    ]
    arrived(left, 1, 2)
    across_chip(left, 1, 3)
    arrived(right, 0, 3)
    across_chip(right, 0, 4)
    for copy in g_copies:
        copy.wait_recv()
    for owner in range(NTP):
        for t in range(2):
            cols = pl.ds((owner * 2 + t) * 128, 128)
            mod[0:4, cols] = gbuf[owner, t]
            mod[4:8, cols] = gbuf[owner, 2 + t]
    amp[...] = gain[...] * (1.0 + mod[1:2, :])
    camp[...] = gain[...] * (1.0 + mod[5:6, :])

    def normed(value, gains, shifts):
        floats = value.astype(F32)
        mean = jnp.mean(floats * floats, axis=-1, keepdims=True)
        return (floats * lax.rsqrt(mean + NORM_EPS) * gains + shifts).astype(BF16)

    ctx_hidden = normed(ctx[...], camp[...], mod[4:5, :])
    ctxkv[0, 0] = jnp.dot(ctx_hidden, wqkv[:, 256:512], preferred_element_type=F32).astype(BF16)
    cz = [
        send(ctxkv.at[0, 0], ctxkv.at[0, d], c_send, c_recv, d, {"z": wrap(z + d, NZ)})
        for d in (8, 7, 9, 6, 10, 5, 11, 4, 12, 3, 13, 2, 14, 1, 15)
    ]
    cz_of = dict(zip((8, 7, 9, 6, 10, 5, 11, 4, 12, 3, 13, 2, 14, 1, 15), cz))

    arrived(across, 0, 4)
    across_chip(across, 0, 5)
    arrived(across, 1, 5)
    across_chip(across, 1, 6)
    remote(lat, rows.at[rows_at((x * NC + 1 - c) * ROWS, ROWS)], p_send.at[0], p_recv.at[0], partner).wait_recv()
    for chip, h, k in [(left, 0, 1), (right, 1, 2), (left, 1, 3), (right, 0, 4), (across, 0, 5), (across, 1, 6)]:
        slot = piece(chip, 1 - c, h)
        remote(slot, slot, p_send.at[k], p_recv.at[k], partner).wait_recv()

    lanes = lax.broadcasted_iota(jnp.int32, (16, 128), 1)
    first = lanes % 64 < 32

    def project(chips):
        for n, chip in enumerate(chips):
            def norm_step(i, carry):
                for g in range(4):
                    src = rows_at(chip * CHIP + i * 64 + g * 16, 16)
                    dst = rows_at(n * CHIP + i * 64 + g * 16, 16)
                    acc = jnp.zeros((16, 128), F32)
                    for j in range(WIDTH // 128):
                        v = rows[src, j * 128 : j * 128 + 128].astype(F32)
                        acc = acc + v * v
                    mean = jnp.sum(acc, axis=1, keepdims=True) * (1.0 / WIDTH)
                    inverse = jnp.broadcast_to(lax.rsqrt(mean + NORM_EPS), (16, 128))
                    for j in range(WIDTH // 128):
                        cols = slice(j * 128, j * 128 + 128)
                        v = rows[src, cols].astype(F32)
                        hid[dst, cols] = (v * inverse * amp[:, cols] + mod[0:1, cols]).astype(BF16)
                return carry

            lax.fori_loop(0, CHIP // 64, norm_step, 0)
        qkv[...] = jnp.dot(hid[...], wqkv[...], preferred_element_type=F32)
        for n, chip in enumerate(chips):
            def turn_step(i, carry):
                for g in range(2):
                    at = rows_at(n * CHIP + i * 32 + g * 16, 16)
                    to = rows_at(chip * CHIP + i * 32 + g * 16, 16)
                    pad = rows_at(chip * CHIP + i * 32 + g * 16 + WINDOW_REACH, 16)
                    cosine, sine = cos_t[to], sin_t[to]
                    for h in range(3):
                        u = qkv[at, h * 128 : h * 128 + 128]
                        swapped = jnp.where(first, pltpu.roll(u, 96, 1), pltpu.roll(u, 32, 1))
                        turned = (u * cosine + swapped * sine).astype(BF16)
                        if h < 2:
                            q[to, h * 128 : h * 128 + 128] = turned
                        else:
                            kv[pad, 0:128] = turned
                    kv[pad, 128:256] = qkv[at, 384:512].astype(BF16)
                return carry

            lax.fori_loop(0, CHIP // 32, turn_step, 0)

    project((0, 3))
    halo = [
        send(kv.at[pl.ds(GROUP, 128)], kv.at[pl.ds(0, 128)], h_send, h_recv, 0, after),
        send(kv.at[pl.ds(128, 128)], kv.at[pl.ds(GROUP + 128, 128)], h_send, h_recv, 1, before),
    ]
    for d in range(1, 8):
        cz_of[d].wait_recv()
    send(ctxkv.at[0, pl.ds(0, 8)], ctxkv.at[1, pl.ds(0, 8)], d_send, d_recv, 0, {"y": up})
    send(ctxkv.at[0, pl.ds(0, 8)], ctxkv.at[2, pl.ds(0, 8)], d_send, d_recv, 3, {"y": down})
    for d in range(8, 16):
        cz_of[d].wait_recv()
    send(ctxkv.at[0, pl.ds(8, 8)], ctxkv.at[2, pl.ds(8, 8)], d_send, d_recv, 1, {"y": down})
    send(ctxkv.at[0, pl.ds(8, 8)], ctxkv.at[1, pl.ds(8, 8)], d_send, d_recv, 2, {"y": up})

    project((1, 2))

    def ctx_arrived(slot, h, k):
        ref = ctxkv.at[slot, pl.ds(h * 8, 8)]
        remote(ref, ref, d_send.at[k], d_recv.at[k], {"y": up}).wait_recv()

    ctx_arrived(1, 0, 0)
    send(ctxkv.at[1, pl.ds(0, 8)], ctxkv.at[3, pl.ds(0, 8)], d_send, d_recv, 4, {"y": up})
    ctx_arrived(2, 1, 1)
    send(ctxkv.at[2, pl.ds(8, 8)], ctxkv.at[3, pl.ds(8, 8)], d_send, d_recv, 5, {"y": down})
    for copy in halo:
        copy.wait_recv()
    ctx_arrived(1, 1, 2)
    ctx_arrived(2, 0, 3)
    ctx_arrived(3, 0, 4)
    ctx_arrived(3, 1, 5)

    nt = (((1,), (1,)), ((), ()))
    factor = HEAD_DIM ** (-0.5) * LOG2E
    last = sp * GROUP - WINDOW_REACH

    def attend(chip):
        begin = chip * CHIP
        at = rows_at(begin, CHIP)
        both = jnp.concatenate([q[at, 0:128], q[at, 128:256]], axis=0)
        window = rows_at(begin, WIN)
        key_at = last + begin + lax.broadcasted_iota(jnp.int32, (1, WIN), 1)
        edge = jnp.where((key_at >= 0) & (key_at < GROUP * NZ * NY), 0.0, MASKED_SCORE)
        bias = band[...] + edge
        near = lax.dot_general(both, kv[window, 0:128], nt, preferred_element_type=F32)
        near = near * factor + jnp.concatenate([bias, bias], axis=0)
        keys = ctxkv[:, :, :, 0:128].reshape(1024, 128)
        values = ctxkv[:, :, :, 128:256].reshape(1024, 128)
        far = lax.dot_general(both, keys, nt, preferred_element_type=F32) * factor
        head = lax.broadcasted_iota(jnp.int32, (2 * CHIP, 1), 0)
        sinks = jnp.where(head < CHIP, sink[0:1, 0:1], sink[0:1, 1:2]) * LOG2E
        top = jnp.maximum(
            jnp.maximum(jnp.max(near, axis=1, keepdims=True), jnp.max(far, axis=1, keepdims=True)), sinks
        )
        near = jnp.exp2(near - top)
        far = jnp.exp2(far - top)
        bottom = (
            jnp.sum(near, axis=1, keepdims=True)
            + jnp.sum(far, axis=1, keepdims=True)
            + jnp.exp2(sinks - top)
        )
        mixed = jnp.dot(near.astype(BF16), kv[window, 128:256], preferred_element_type=F32)
        mixed = mixed + jnp.dot(far.astype(BF16), values, preferred_element_type=F32)
        mixed = (mixed / bottom).astype(BF16)
        for h in range(2):
            for core in range(NC):
                begin = h * CHIP + core * ROWS
                att[chip, core, :, h * 128 : h * 128 + 128] = mixed[begin : begin + ROWS]
        return send(att.at[chip, 1 - c], att_mate.at[chip], m_send, m_recv, chip, partner)

    def product(chip, h):
        cols = slice(h * 1024, h * 1024 + 1024)
        return jnp.dot(att[chip, c], wo[:, cols], preferred_element_type=F32) + jnp.dot(
            att_mate[chip], wo_mate[:, cols], preferred_element_type=F32
        )

    def around(src, dst, k, to):
        return send(src, dst, s_send, s_recv, k, {"x": to})

    remote(wo, wo_mate, m_send.at[4], m_recv.at[4], partner).wait_recv()
    attend(across).wait_recv()
    opp_src[0] = product(across, 0).astype(BF16)
    first_left = around(opp_src.at[0], opp_left, 0, right)
    opp_src[1] = product(across, 1).astype(BF16)
    first_right = around(opp_src.at[1], opp_right, 1, left)
    right_mate = attend(right)
    left_mate = attend(left)
    right_mate.wait_recv()
    right_src[1] = product(right, 1).astype(BF16)
    r1 = around(right_src.at[1], from_left.at[1], 2, right)
    left_mate.wait_recv()
    left_src[0] = product(left, 0).astype(BF16)
    l0 = around(left_src.at[0], from_right.at[0], 3, left)
    own_mate = attend(x)
    right_part = product(right, 0)
    first_left.wait_recv()
    right_src[0] = (right_part + opp_left[...].astype(F32)).astype(BF16)
    r0 = around(right_src.at[0], from_left.at[0], 4, right)
    left_part = product(left, 1)
    first_right.wait_recv()
    left_src[1] = (left_part + opp_right[...].astype(F32)).astype(BF16)
    l1 = around(left_src.at[1], from_right.at[1], 5, left)
    own_mate.wait_recv()
    totals = [product(x, h) for h in range(2)]
    for copy in (r1, l0, r0, l1):
        copy.wait_recv()
    for h in range(2):
        cols = slice(h * 1024, h * 1024 + 1024)
        total = totals[h] + from_left[h].astype(F32) + from_right[h].astype(F32)
        out_ref[:, cols] = (lat[:, cols].astype(F32) + mod[2:3, cols] * total).astype(BF16)
    for copy in sent:
        copy.wait_send()


def shards(
    latent,
    condition,
    context_condition,
    context,
    norm_gain,
    shift_weight,
    scale_weight,
    gate_weight,
    query_weight,
    key_matrix,
    value_matrix,
    sink_logit_head,
    out_weight,
):
    lanes = np.arange(HEAD_DIM) % 32
    freq = (10000.0 ** (-(2.0 * lanes) / 64.0)).astype(np.float32)[None]
    vm = pltpu.VMEM
    dma = pltpu.SemaphoreType.DMA
    half = (2, ROWS, WIDTH // 2)
    return pl.pallas_call(
        block_kernel,
        out_shape=jax.ShapeDtypeStruct((ROWS, WIDTH), BF16),
        in_specs=[pl.BlockSpec(memory_space=pl.ANY)] * 14,
        out_specs=pl.BlockSpec(memory_space=pltpu.VMEM),
        scratch_shapes=[
            vm((ROWS, WIDTH), BF16), vm((CTX_ROWS, WIDTH), BF16), vm((1, WIDTH), F32),
            vm((1, 32), F32), vm((1, 32), F32),
            vm((32, 256), BF16), vm((32, 256), BF16), vm((32, 256), BF16),
            vm((WIDTH, 512), BF16), vm((1, 2), F32), vm((256, WIDTH), BF16), vm((1, 128), F32),
            vm((GROUP, WIDTH), BF16),
            vm((4, 4, 128), F32), vm((NY, 4, 128), F32), vm((4, 128), F32), vm((NZ, 4, 128), F32),
            vm((4, 128), F32), vm((NTP, NY, 4, 128), F32),
            vm((8, WIDTH), F32), vm((1, WIDTH), F32), vm((1, WIDTH), F32),
            vm((GROUP, 128), F32), vm((GROUP, 128), F32), vm((CHIP, WIN), F32),
            vm((2 * CHIP, WIDTH), BF16), vm((2 * CHIP, 512), F32),
            vm((GROUP, 256), BF16), vm((GROUP + 256 + 64, 256), BF16),
            vm((NY, NZ, CTX_ROWS, 256), BF16),
            vm((NX, NC, ROWS, 256), BF16), vm((NX, ROWS, 256), BF16), vm((256, WIDTH), BF16),
            vm(half, BF16), vm(half, BF16), vm(half, BF16),
            vm(half[1:], BF16), vm(half[1:], BF16), vm(half, BF16), vm(half, BF16),
            dma((15,)),
            dma((NY,)), dma((NY,)), dma((NZ,)), dma((NZ,)), dma((31,)), dma((31,)),
            dma((6,)), dma((6,)), dma((7,)), dma((7,)),
            dma((NZ,)), dma((NZ,)), dma((6,)), dma((6,)), dma((2,)), dma((2,)),
            dma((5,)), dma((5,)), dma((6,)), dma((6,)),
        ],
        compiler_params=pltpu.CompilerParams(
            collective_id=0, has_side_effects=True, vmem_limit_bytes=62 * 1024 * 1024
        ),
        cost_estimate=pl.CostEstimate(flops=10**9, bytes_accessed=10**7, transcendentals=0),
        name="block",
    )(
        latent, context, norm_gain.reshape(1, -1), condition.reshape(1, -1),
        context_condition.reshape(1, -1), shift_weight, scale_weight, gate_weight,
        query_weight, key_matrix, value_matrix, sink_logit_head.reshape(1, -1), out_weight,
        jnp.asarray(freq),
    )


def solution(mesh):
    torus = Mesh(mesh.devices.reshape(NZ, NY, NX, NC), ALL)
    return jax.shard_map(
        shards,
        mesh=torus,
        in_specs=(
            P(ALL, None),
            P(SP),
            P(SP),
            P(SP, None),
            P(),
            P(SP, TP),
            P(SP, TP),
            P(SP, TP),
            P(None, TP),
            P(None, TP),
            P(None, TP),
            P(TP),
            P(TP, None),
        ),
        out_specs=P(ALL, None),
        check_vma=False,
    )
```

```python
import functools

import jax
import jax.numpy as jnp
import numpy as np
from jax import lax
from jax.experimental import pallas as pl
from jax.experimental.pallas import tpu as pltpu
from jax.sharding import Mesh
from jax.sharding import PartitionSpec as P

HEAD_DIM = 128
WINDOW_REACH = 128
GRID_W = 64
SP = ("z", "y")
TP = ("x", "c")
ALL = ("z", "y", "x", "c")
MESH = pl.DeviceIdType.MESH

NORM_EPS = 1e-05
MASKED_SCORE = -1e30
LOG2E = 1.4426950408889634
NZ, NY, NX, NC = 16, 4, 4, 2
NTP = NX * NC
WIDTH = 2048
ROWS = 96
GROUP = ROWS * NTP
CHIP = ROWS * NC
CTX_ROWS = 16
WIN = 512
F32 = jnp.float32
BF16 = jnp.bfloat16
PLANE = [
    (dy, dx, dc)
    for dy in range(NY)
    for dx in range(NX)
    for dc in range(NC)
    if (dy, dx, dc) != (0, 0, 0)
]


def wrap(value, size):
    return lax.rem(value + size, size)


def remote(src, dst, send, recv, device):
    return pltpu.make_async_remote_copy(
        src_ref=src,
        dst_ref=dst,
        send_sem=send,
        recv_sem=recv,
        device_id=device,
        device_id_type=MESH,
    )


def rows_at(start, count):
    return pl.ds(pl.multiple_of(start, 16), count)


def block_kernel(
    lat_hbm, ctx_hbm, gain_hbm, cond_hbm, cctx_hbm, sw_hbm, cw_hbm, gw_hbm,
    wq_hbm, wk_hbm, wv_hbm, sink_hbm, wo_hbm, freq_hbm,
    out_ref,
    lat, cr, gain, cond, cctx, sw, cw, gw, wqkv, sink, wo, freq,
    rows, parts, ybuf, zsrc, zbuf, csrc, gsrc, gbuf, mod, amp, camp,
    cos_t, sin_t, band, hid, chid, qkv, q, kv, ctxkv,
    att, att_mate, wo_mate, opp_src, right_src, left_src, opp_left, opp_right, from_left, from_right,
    l_sem, y_send, y_recv, z_send, z_recv, g_send, g_recv, a_send, a_recv, p_send, p_recv,
    e_send, e_recv, f_send, f_recv, d_send, d_recv, h_send, h_recv, m_send, m_recv, s_send, s_recv,
):
    z, y, x, c = (lax.axis_index(a) for a in ALL)
    tp = x * NC + c
    sp = z * NY + y
    right, left, across = wrap(x + 1, NX), wrap(x - 1, NX), wrap(x + 2, NX)
    up, down = wrap(y + 1, NY), wrap(y - 1, NY)
    partner = {"c": 1 - c}
    after = {"z": wrap(z + (y + 1) // NY, NZ), "y": up}
    before = {"z": wrap(z - (NY - y) // NY, NZ), "y": down}

    def plane_peer(dy, dx, dc):
        return {"y": wrap(y + dy, NY), "x": wrap(x + dx, NX), "c": wrap(c + dc, NC)}

    barrier = pltpu.get_barrier_semaphore()
    peers = [{"z": wrap(z + d, NZ)} for d in (1, -1, 2, -2, 4, -4)]
    peers += [plane_peer(*p) for p in PLANE] + [after, before]
    for peer in peers:
        pl.semaphore_signal(barrier, inc=1, device_id=peer, device_id_type=MESH)
    pairs = [
        (cond_hbm, cond), (cctx_hbm, cctx), (sw_hbm, sw), (cw_hbm, cw), (gw_hbm, gw),
        (lat_hbm, lat), (freq_hbm, freq), (gain_hbm, gain), (sink_hbm, sink),
        (ctx_hbm.at[:, pl.ds(0, 1024)], cr.at[0, z]), (ctx_hbm.at[:, pl.ds(1024, 1024)], cr.at[1, z]),
        (wq_hbm, wqkv.at[:, pl.ds(0, 256)]), (wk_hbm, wqkv.at[:, pl.ds(256, 128)]),
        (wv_hbm, wqkv.at[:, pl.ds(384, 128)]), (wo_hbm, wo),
        (lat_hbm, rows.at[rows_at(tp * ROWS, ROWS)]),
    ]
    local = [pltpu.make_async_copy(s, d, l_sem.at[k]) for k, (s, d) in enumerate(pairs)]
    for copy in local:
        copy.start()

    for copy in local[:5]:
        copy.wait()
    row = lax.broadcasted_iota(jnp.int32, (8, 32), 0)
    vectors = jnp.where(
        row == 0, jnp.broadcast_to(cond[...], (8, 32)), jnp.broadcast_to(cctx[...], (8, 32))
    )
    active = (vectors / (1.0 + jnp.exp(-vectors))).astype(BF16)
    shift_part = jnp.dot(active, sw[...], preferred_element_type=F32)
    scale_part = jnp.dot(active, cw[...], preferred_element_type=F32)
    gate_part = jnp.dot(active, gw[...], preferred_element_type=F32)
    for t in range(2):
        cols = slice(t * 128, t * 128 + 128)
        parts[t] = jnp.concatenate(
            [shift_part[0:1, cols], scale_part[0:1, cols], gate_part[0:1, cols], gate_part[0:1, cols]],
            axis=0,
        )
        parts[2 + t] = jnp.concatenate(
            [shift_part[1:2, cols], scale_part[1:2, cols], scale_part[1:2, cols], scale_part[1:2, cols]],
            axis=0,
        )
    for copy in local[5:]:
        copy.wait()

    lane = lax.broadcasted_iota(jnp.int32, (64, 128), 1)
    sign = jnp.where(lane % 64 < 32, -1.0, 1.0)
    col_angle = lax.broadcasted_iota(jnp.int32, (64, 128), 0).astype(F32) * freq[...]
    col_cos, col_sin = jnp.cos(col_angle), jnp.sin(col_angle) * sign
    row_ids = sp * (GROUP // GRID_W) + lax.broadcasted_iota(jnp.int32, (16, 128), 0)
    row_angle = row_ids.astype(F32) * freq[...]
    row_cos, row_sin = jnp.cos(row_angle), jnp.sin(row_angle) * sign[0:16]
    for i in range(GROUP // GRID_W):
        block = slice(i * GRID_W, i * GRID_W + GRID_W)
        cos_t[block] = jnp.where(lane < 64, jnp.broadcast_to(row_cos[i : i + 1], (64, 128)), col_cos)
        sin_t[block] = jnp.where(lane < 64, jnp.broadcast_to(row_sin[i : i + 1], (64, 128)), col_sin)
    gap = lax.broadcasted_iota(jnp.int32, (CHIP, WIN), 1) - lax.broadcasted_iota(
        jnp.int32, (CHIP, WIN), 0
    )
    band[...] = jnp.where((gap >= 0) & (gap <= 2 * WINDOW_REACH), 0.0, MASKED_SCORE)
    kv[1024:, :] = jnp.zeros((64, 256), BF16)
    pl.semaphore_wait(barrier, len(peers))

    sent = []

    def send(src, dst, s_sem, r_sem, k, to):
        copy = remote(src, dst, s_sem.at[k], r_sem.at[k], to)
        copy.start()
        sent.append(copy)
        return copy

    y_copies = [
        send(parts.at[wrap(y + d, NY)], ybuf.at[d], y_send, y_recv, d, {"y": wrap(y + d, NY)})
        for d in range(1, NY)
    ]

    def piece(chip, core, h):
        return rows.at[rows_at((chip * NC + core) * ROWS + h * 48, 48)]

    def along(chip, h, k, to):
        source = lat.at[pl.ds(h * 48, 48)] if chip is None else piece(chip, c, h)
        slot = piece(x if chip is None else chip, c, h)
        send(source, slot, a_send, a_recv, k, {"x": to})

    def across_chip(chip, h, k):
        send(piece(chip, c, h), piece(chip, c, h), p_send, p_recv, k, partner)

    def arrived(chip, h, k):
        slot = piece(chip, c, h)
        remote(slot, slot, a_send.at[k], a_recv.at[k], {"x": right}).wait_recv()

    along(None, 0, 0, right)
    along(None, 1, 1, left)
    along(None, 1, 2, right)
    along(None, 0, 3, left)
    own_slot = rows.at[rows_at(tp * ROWS, ROWS)]
    send(lat, own_slot, p_send, p_recv, 0, partner)
    send(wo, wo_mate, m_send, m_recv, 4, partner)

    side = 1 - 2 * c

    def ctx_send(block, k, to):
        slot = cr.at[c, block]
        send(slot, slot, e_send, e_recv, k, {"z": to})

    def ctx_came(block, k):
        slot = cr.at[c, block]
        remote(slot, slot, e_send.at[k], e_recv.at[k], partner).wait_recv()
        send(slot, slot, f_send, f_recv, k, partner)

    def ctx_spread(block, n):
        ctx_send(block, 3 + n, wrap(z + 1, NZ))
        ctx_send(block, 7 + n, wrap(z - 1, NZ))
        ctx_send(block, 11 + n, wrap(z + 2 * side, NZ))

    ctx_send(z, 0, wrap(z + 4, NZ))
    ctx_send(z, 1, wrap(z - 4, NZ))
    ctx_spread(z, 0)

    for copy in y_copies:
        copy.wait_recv()
    zsrc[...] = parts[y] + ybuf[1] + ybuf[2] + ybuf[3]

    def z_send_to(src, slot, k, d):
        return send(src, zbuf.at[slot], z_send, z_recv, k, {"z": wrap(z + d, NZ)})

    low = z_send_to(zsrc, 1, 0, 4)
    high = z_send_to(zsrc, 2, 1, -4)

    arrived(left, 0, 0)
    along(left, 0, 4, right)
    across_chip(left, 0, 1)
    arrived(right, 1, 1)
    along(right, 1, 5, left)
    across_chip(right, 1, 2)

    low.wait_recv()
    far_sum = z_send_to(zbuf.at[1], 3, 2, 4)
    high.wait_recv()
    ctx_came(wrap(z - 4, NZ), 0)
    ctx_came(wrap(z + 4, NZ), 1)
    ctx_send(wrap(z - 4 * side, NZ), 2, wrap(z + 4 * side, NZ))
    ctx_spread(wrap(z - 4, NZ), 1)
    ctx_spread(wrap(z + 4, NZ), 2)
    far_sum.wait_recv()
    csrc[...] = zsrc[...] + zbuf[1] + zbuf[2] + zbuf[3]
    near_sums = [z_send_to(csrc, 4, 3, 1), z_send_to(csrc, 5, 4, -1), z_send_to(csrc, 6, 5, -2)]
    ctx_came(wrap(z + 8, NZ), 2)
    ctx_spread(wrap(z + 8, NZ), 3)
    arrived(left, 1, 2)
    across_chip(left, 1, 3)
    arrived(right, 0, 3)
    across_chip(right, 0, 4)
    for copy in near_sums:
        copy.wait_recv()
    total = csrc[...] + zbuf[4] + zbuf[5] + zbuf[6]
    gsrc[...] = total
    gbuf[tp, y] = total
    g_copies = [
        send(gsrc, gbuf.at[tp, y], g_send, g_recv, k, plane_peer(*p)) for k, p in enumerate(PLANE)
    ]
    for n in range(4):
        step = (0, -4, 4, 8)[n]
        ctx_came(wrap(z - 1 + step, NZ), 3 + n)
        ctx_came(wrap(z + 1 + step, NZ), 7 + n)
        ctx_came(wrap(z - 2 * side + step, NZ), 11 + n)
    arrived(across, 0, 4)
    across_chip(across, 0, 5)
    arrived(across, 1, 5)
    across_chip(across, 1, 6)
    for copy in g_copies:
        copy.wait_recv()
    for owner in range(NTP):
        for t in range(2):
            cols = pl.ds((owner * 2 + t) * 128, 128)
            mod[0:4, cols] = gbuf[owner, t]
            mod[4:8, cols] = gbuf[owner, 2 + t]
    amp[...] = gain[...] * (1.0 + mod[1:2, :])
    camp[...] = gain[...] * (1.0 + mod[5:6, :])

    for k in range(15):
        slot = cr.at[1 - c, z]
        remote(slot, slot, f_send.at[k], f_recv.at[k], partner).wait_recv()

    def normed(load, store, gains, shifts):
        acc = jnp.zeros((16, 128), F32)
        for j in range(WIDTH // 128):
            v = load(j).astype(F32)
            acc = acc + v * v
        mean = jnp.sum(acc, axis=1, keepdims=True) * (1.0 / WIDTH)
        inverse = jnp.broadcast_to(lax.rsqrt(mean + NORM_EPS), (16, 128))
        for j in range(WIDTH // 128):
            cols = slice(j * 128, j * 128 + 128)
            v = load(j).astype(F32)
            store(cols, (v * inverse * gains[:, cols] + shifts[:, cols]).astype(BF16))

    def ctx_step(i, carry):
        for g in range(4):
            block = i * 4 + g
            dst = rows_at(block * CTX_ROWS, CTX_ROWS)

            def load(j):
                return cr[j // 8, block, :, (j % 8) * 128 : (j % 8) * 128 + 128]

            def store(cols, value):
                chid[dst, cols] = value

            normed(load, store, camp, mod[4:5, :])
        return carry

    lax.fori_loop(0, NZ // 4, ctx_step, 0)
    ctxkv[0] = jnp.dot(chid[...], wqkv[:, 256:512], preferred_element_type=F32).astype(BF16)

    def ctx_half(slot, h):
        return ctxkv.at[slot, pl.ds(h * 128, 128)]

    send(ctx_half(0, 0), ctx_half(1, 0), d_send, d_recv, 0, {"y": up})
    send(ctx_half(0, 1), ctx_half(2, 1), d_send, d_recv, 1, {"y": down})
    send(ctx_half(0, 1), ctx_half(1, 1), d_send, d_recv, 2, {"y": up})
    send(ctx_half(0, 0), ctx_half(2, 0), d_send, d_recv, 3, {"y": down})

    remote(lat, rows.at[rows_at((x * NC + 1 - c) * ROWS, ROWS)], p_send.at[0], p_recv.at[0], partner).wait_recv()
    for chip, h, k in [(left, 0, 1), (right, 1, 2), (left, 1, 3), (right, 0, 4), (across, 0, 5), (across, 1, 6)]:
        slot = piece(chip, 1 - c, h)
        remote(slot, slot, p_send.at[k], p_recv.at[k], partner).wait_recv()

    lanes = lax.broadcasted_iota(jnp.int32, (16, 128), 1)
    first = lanes % 64 < 32

    def project(chips):
        for n, chip in enumerate(chips):
            def norm_step(i, carry):
                for g in range(4):
                    src = rows_at(chip * CHIP + i * 64 + g * 16, 16)
                    dst = rows_at(n * CHIP + i * 64 + g * 16, 16)

                    def load(j):
                        return rows[src, j * 128 : j * 128 + 128]

                    def store(cols, value):
                        hid[dst, cols] = value

                    normed(load, store, amp, mod[0:1, :])
                return carry

            lax.fori_loop(0, CHIP // 64, norm_step, 0)
        qkv[...] = jnp.dot(hid[...], wqkv[...], preferred_element_type=F32)
        for n, chip in enumerate(chips):
            def turn_step(i, carry):
                for g in range(2):
                    at = rows_at(n * CHIP + i * 32 + g * 16, 16)
                    to = rows_at(chip * CHIP + i * 32 + g * 16, 16)
                    pad = rows_at(chip * CHIP + i * 32 + g * 16 + WINDOW_REACH, 16)
                    cosine, sine = cos_t[to], sin_t[to]
                    for h in range(3):
                        u = qkv[at, h * 128 : h * 128 + 128]
                        swapped = jnp.where(first, pltpu.roll(u, 96, 1), pltpu.roll(u, 32, 1))
                        turned = (u * cosine + swapped * sine).astype(BF16)
                        if h < 2:
                            q[to, h * 128 : h * 128 + 128] = turned
                        else:
                            kv[pad, 0:128] = turned
                    kv[pad, 128:256] = qkv[at, 384:512].astype(BF16)
                return carry

            lax.fori_loop(0, CHIP // 32, turn_step, 0)

    project((0, 3))
    halo = [
        send(kv.at[pl.ds(GROUP, 128)], kv.at[pl.ds(0, 128)], h_send, h_recv, 0, after),
        send(kv.at[pl.ds(128, 128)], kv.at[pl.ds(GROUP + 128, 128)], h_send, h_recv, 1, before),
    ]
    project((1, 2))

    def ctx_arrived(slot, h, k):
        ref = ctx_half(slot, h)
        remote(ref, ref, d_send.at[k], d_recv.at[k], {"y": up}).wait_recv()

    ctx_arrived(1, 0, 0)
    send(ctx_half(1, 0), ctx_half(3, 0), d_send, d_recv, 4, {"y": up})
    ctx_arrived(2, 1, 1)
    send(ctx_half(2, 1), ctx_half(3, 1), d_send, d_recv, 5, {"y": down})
    for copy in halo:
        copy.wait_recv()
    ctx_arrived(1, 1, 2)
    ctx_arrived(2, 0, 3)
    ctx_arrived(3, 0, 4)
    ctx_arrived(3, 1, 5)

    nt = (((1,), (1,)), ((), ()))
    factor = HEAD_DIM ** (-0.5) * LOG2E
    last = sp * GROUP - WINDOW_REACH

    def attend(chip):
        begin = chip * CHIP
        at = rows_at(begin, CHIP)
        both = jnp.concatenate([q[at, 0:128], q[at, 128:256]], axis=0)
        window = rows_at(begin, WIN)
        key_at = last + begin + lax.broadcasted_iota(jnp.int32, (1, WIN), 1)
        edge = jnp.where((key_at >= 0) & (key_at < GROUP * NZ * NY), 0.0, MASKED_SCORE)
        bias = band[...] + edge
        near = lax.dot_general(both, kv[window, 0:128], nt, preferred_element_type=F32)
        near = near * factor + jnp.concatenate([bias, bias], axis=0)
        keys = ctxkv[:, :, 0:128].reshape(1024, 128)
        values = ctxkv[:, :, 128:256].reshape(1024, 128)
        far = lax.dot_general(both, keys, nt, preferred_element_type=F32) * factor
        head = lax.broadcasted_iota(jnp.int32, (2 * CHIP, 1), 0)
        sinks = jnp.where(head < CHIP, sink[0:1, 0:1], sink[0:1, 1:2]) * LOG2E
        top = jnp.maximum(
            jnp.maximum(jnp.max(near, axis=1, keepdims=True), jnp.max(far, axis=1, keepdims=True)), sinks
        )
        near = jnp.exp2(near - top)
        far = jnp.exp2(far - top)
        bottom = (
            jnp.sum(near, axis=1, keepdims=True)
            + jnp.sum(far, axis=1, keepdims=True)
            + jnp.exp2(sinks - top)
        )
        mixed = jnp.dot(near.astype(BF16), kv[window, 128:256], preferred_element_type=F32)
        mixed = mixed + jnp.dot(far.astype(BF16), values, preferred_element_type=F32)
        mixed = (mixed / bottom).astype(BF16)
        for h in range(2):
            for core in range(NC):
                begin = h * CHIP + core * ROWS
                att[chip, core, :, h * 128 : h * 128 + 128] = mixed[begin : begin + ROWS]
        return send(att.at[chip, 1 - c], att_mate.at[chip], m_send, m_recv, chip, partner)

    def product(chip, h):
        cols = slice(h * 1024, h * 1024 + 1024)
        return jnp.dot(att[chip, c], wo[:, cols], preferred_element_type=F32) + jnp.dot(
            att_mate[chip], wo_mate[:, cols], preferred_element_type=F32
        )

    def around(src, dst, k, to):
        return send(src, dst, s_send, s_recv, k, {"x": to})

    remote(wo, wo_mate, m_send.at[4], m_recv.at[4], partner).wait_recv()
    attend(across).wait_recv()
    opp_src[0] = product(across, 0).astype(BF16)
    first_left = around(opp_src.at[0], opp_left, 0, right)
    opp_src[1] = product(across, 1).astype(BF16)
    first_right = around(opp_src.at[1], opp_right, 1, left)
    right_mate = attend(right)
    left_mate = attend(left)
    right_mate.wait_recv()
    right_src[1] = product(right, 1).astype(BF16)
    r1 = around(right_src.at[1], from_left.at[1], 2, right)
    left_mate.wait_recv()
    left_src[0] = product(left, 0).astype(BF16)
    l0 = around(left_src.at[0], from_right.at[0], 3, left)
    own_mate = attend(x)
    right_part = product(right, 0)
    first_left.wait_recv()
    right_src[0] = (right_part + opp_left[...].astype(F32)).astype(BF16)
    r0 = around(right_src.at[0], from_left.at[0], 4, right)
    left_part = product(left, 1)
    first_right.wait_recv()
    left_src[1] = (left_part + opp_right[...].astype(F32)).astype(BF16)
    l1 = around(left_src.at[1], from_right.at[1], 5, left)
    own_mate.wait_recv()
    totals = [product(x, h) for h in range(2)]
    for copy in (r1, l0, r0, l1):
        copy.wait_recv()
    for h in range(2):
        cols = slice(h * 1024, h * 1024 + 1024)
        total = totals[h] + from_left[h].astype(F32) + from_right[h].astype(F32)
        out_ref[:, cols] = (lat[:, cols].astype(F32) + mod[2:3, cols] * total).astype(BF16)
    for copy in sent:
        copy.wait_send()


def shards(
    latent,
    condition,
    context_condition,
    context,
    norm_gain,
    shift_weight,
    scale_weight,
    gate_weight,
    query_weight,
    key_matrix,
    value_matrix,
    sink_logit_head,
    out_weight,
):
    lanes = np.arange(HEAD_DIM) % 32
    freq = (10000.0 ** (-(2.0 * lanes) / 64.0)).astype(np.float32)[None]
    vm = pltpu.VMEM
    dma = pltpu.SemaphoreType.DMA
    half = (2, ROWS, WIDTH // 2)
    return pl.pallas_call(
        block_kernel,
        out_shape=jax.ShapeDtypeStruct((ROWS, WIDTH), BF16),
        in_specs=[pl.BlockSpec(memory_space=pl.ANY)] * 14,
        out_specs=pl.BlockSpec(memory_space=pltpu.VMEM),
        scratch_shapes=[
            vm((ROWS, WIDTH), BF16), vm((2, NZ, CTX_ROWS, WIDTH // 2), BF16), vm((1, WIDTH), F32),
            vm((1, 32), F32), vm((1, 32), F32),
            vm((32, 256), BF16), vm((32, 256), BF16), vm((32, 256), BF16),
            vm((WIDTH, 512), BF16), vm((1, 2), F32), vm((256, WIDTH), BF16), vm((1, 128), F32),
            vm((GROUP, WIDTH), BF16),
            vm((4, 4, 128), F32), vm((NY, 4, 128), F32), vm((4, 128), F32), vm((7, 4, 128), F32),
            vm((4, 128), F32), vm((4, 128), F32), vm((NTP, NY, 4, 128), F32),
            vm((8, WIDTH), F32), vm((1, WIDTH), F32), vm((1, WIDTH), F32),
            vm((GROUP, 128), F32), vm((GROUP, 128), F32), vm((CHIP, WIN), F32),
            vm((2 * CHIP, WIDTH), BF16), vm((NZ * CTX_ROWS, WIDTH), BF16), vm((2 * CHIP, 512), F32),
            vm((GROUP, 256), BF16), vm((GROUP + 256 + 64, 256), BF16),
            vm((NY, NZ * CTX_ROWS, 256), BF16),
            vm((NX, NC, ROWS, 256), BF16), vm((NX, ROWS, 256), BF16), vm((256, WIDTH), BF16),
            vm(half, BF16), vm(half, BF16), vm(half, BF16),
            vm(half[1:], BF16), vm(half[1:], BF16), vm(half, BF16), vm(half, BF16),
            dma((16,)),
            dma((NY,)), dma((NY,)), dma((6,)), dma((6,)), dma((31,)), dma((31,)),
            dma((6,)), dma((6,)), dma((7,)), dma((7,)),
            dma((15,)), dma((15,)), dma((15,)), dma((15,)), dma((6,)), dma((6,)), dma((2,)), dma((2,)),
            dma((5,)), dma((5,)), dma((6,)), dma((6,)),
        ],
        compiler_params=pltpu.CompilerParams(
            collective_id=0, has_side_effects=True, vmem_limit_bytes=62 * 1024 * 1024
        ),
        cost_estimate=pl.CostEstimate(flops=10**9, bytes_accessed=10**7, transcendentals=0),
        name="block",
    )(
        latent, context, norm_gain.reshape(1, -1), condition.reshape(1, -1),
        context_condition.reshape(1, -1), shift_weight, scale_weight, gate_weight,
        query_weight, key_matrix, value_matrix, sink_logit_head.reshape(1, -1), out_weight,
        jnp.asarray(freq),
    )


def solution(mesh):
    torus = Mesh(mesh.devices.reshape(NZ, NY, NX, NC), ALL)
    return jax.shard_map(
        shards,
        mesh=torus,
        in_specs=(
            P(ALL, None),
            P(SP),
            P(SP),
            P(SP, None),
            P(),
            P(SP, TP),
            P(SP, TP),
            P(SP, TP),
            P(None, TP),
            P(None, TP),
            P(None, TP),
            P(TP),
            P(TP, None),
        ),
        out_specs=P(ALL, None),
        check_vma=False,
    )
```

```python
import functools

import jax
import jax.numpy as jnp
import numpy as np
from jax import lax
from jax.experimental import pallas as pl
from jax.experimental.pallas import tpu as pltpu
from jax.sharding import Mesh
from jax.sharding import PartitionSpec as P

HEAD_DIM = 128
WINDOW_REACH = 128
GRID_W = 64
SP = ("z", "y")
TP = ("x", "c")
ALL = ("z", "y", "x", "c")
MESH = pl.DeviceIdType.MESH

NORM_EPS = 1e-05
MASKED_SCORE = -1e30
LOG2E = 1.4426950408889634
NZ, NY, NX, NC = 16, 4, 4, 2
NTP = NX * NC
WIDTH = 2048
ROWS = 96
GROUP = ROWS * NTP
CHIP = ROWS * NC
CTX_ROWS = 16
WIN = 512
F32 = jnp.float32
BF16 = jnp.bfloat16
PLANE = [
    (dy, dx, dc)
    for dy in (2, 1, 3, 0)
    for dx in (2, 1, 3, 0)
    for dc in (1, 0)
    if (dy, dx, dc) != (0, 0, 0)
]


def wrap(value, size):
    return lax.rem(value + size, size)


def remote(src, dst, send, recv, device):
    return pltpu.make_async_remote_copy(
        src_ref=src,
        dst_ref=dst,
        send_sem=send,
        recv_sem=recv,
        device_id=device,
        device_id_type=MESH,
    )


def rows_at(start, count):
    return pl.ds(pl.multiple_of(start, 16), count)


def block_kernel(
    lat_hbm, ctx_hbm, gain_hbm, cond_hbm, cctx_hbm, sw_hbm, cw_hbm, gw_hbm,
    wq_hbm, wk_hbm, wv_hbm, sink_hbm, wo_hbm, freq_hbm,
    out_ref,
    lat, cr, gain, cond, cctx, sw, cw, gw, wqkv, sink, wo, freq,
    rows, parts, nbuf, zsrc, zbuf, gsrc, gbuf, mod, amp, camp,
    cos_t, sin_t, band, hid, chid, qkv, q, kv, ctxkv,
    att, att_mate, wo_mate, opp_src, right_src, left_src, opp_left, opp_right, from_left, from_right,
    l_sem, n_send, n_recv, z_send, z_recv, g_send, g_recv, a_send, a_recv, p_send, p_recv,
    e_send, e_recv, f_send, f_recv, o_send, o_recv, d_send, d_recv, h_send, h_recv, m_send, m_recv, s_send, s_recv,
):
    z, y, x, c = (lax.axis_index(a) for a in ALL)
    tp = x * NC + c
    sp = z * NY + y
    right, left, across = wrap(x + 1, NX), wrap(x - 1, NX), wrap(x + 2, NX)
    up, down = wrap(y + 1, NY), wrap(y - 1, NY)
    partner = {"c": 1 - c}
    after = {"z": wrap(z + (y + 1) // NY, NZ), "y": up}
    before = {"z": wrap(z - (NY - y) // NY, NZ), "y": down}

    def plane_peer(dy, dx, dc):
        return {"y": wrap(y + dy, NY), "x": wrap(x + dx, NX), "c": wrap(c + dc, NC)}

    barrier = pltpu.get_barrier_semaphore()
    peers = [{"z": wrap(z + d, NZ)} for d in (1, -1, 2, -2, 4, -4)]
    peers += [
        {"z": wrap(z + d, NZ), "y": wrap(y + e, NY)} for d in (1, -1, 2, -2) for e in range(1, NY)
    ]
    peers += [plane_peer(*p) for p in PLANE] + [after, before]
    for peer in peers:
        pl.semaphore_signal(barrier, inc=1, device_id=peer, device_id_type=MESH)
    pairs = [
        (cond_hbm, cond), (cctx_hbm, cctx), (sw_hbm, sw), (cw_hbm, cw), (gw_hbm, gw),
        (lat_hbm, lat), (freq_hbm, freq), (gain_hbm, gain), (sink_hbm, sink),
        (ctx_hbm.at[:, pl.ds(0, 1024)], cr.at[0, 0, z]),
        (ctx_hbm.at[:, pl.ds(1024, 1024)], cr.at[1, 0, z]),
        (wq_hbm, wqkv.at[:, pl.ds(0, 256)]), (wk_hbm, wqkv.at[:, pl.ds(256, 128)]),
        (wv_hbm, wqkv.at[:, pl.ds(384, 128)]), (wo_hbm, wo),
        (lat_hbm, rows.at[rows_at(tp * ROWS, ROWS)]),
    ]
    local = [pltpu.make_async_copy(s, d, l_sem.at[k]) for k, (s, d) in enumerate(pairs)]
    for copy in local:
        copy.start()

    for copy in local[:5]:
        copy.wait()
    row = lax.broadcasted_iota(jnp.int32, (8, 32), 0)
    vectors = jnp.where(
        row == 0, jnp.broadcast_to(cond[...], (8, 32)), jnp.broadcast_to(cctx[...], (8, 32))
    )
    active = (vectors / (1.0 + jnp.exp(-vectors))).astype(BF16)
    shift_part = jnp.dot(active, sw[...], preferred_element_type=F32)
    scale_part = jnp.dot(active, cw[...], preferred_element_type=F32)
    gate_part = jnp.dot(active, gw[...], preferred_element_type=F32)
    for t in range(2):
        cols = slice(t * 128, t * 128 + 128)
        parts[t] = jnp.concatenate(
            [shift_part[0:1, cols], scale_part[0:1, cols], gate_part[0:1, cols], gate_part[0:1, cols]],
            axis=0,
        )
        parts[2 + t] = jnp.concatenate(
            [shift_part[1:2, cols], scale_part[1:2, cols], scale_part[1:2, cols], scale_part[1:2, cols]],
            axis=0,
        )
    for copy in local[5:]:
        copy.wait()

    lane = lax.broadcasted_iota(jnp.int32, (64, 128), 1)
    sign = jnp.where(lane % 64 < 32, -1.0, 1.0)
    col_angle = lax.broadcasted_iota(jnp.int32, (64, 128), 0).astype(F32) * freq[...]
    col_cos, col_sin = jnp.cos(col_angle), jnp.sin(col_angle) * sign
    row_ids = sp * (GROUP // GRID_W) + lax.broadcasted_iota(jnp.int32, (16, 128), 0)
    row_angle = row_ids.astype(F32) * freq[...]
    row_cos, row_sin = jnp.cos(row_angle), jnp.sin(row_angle) * sign[0:16]
    for i in range(GROUP // GRID_W):
        block = slice(i * GRID_W, i * GRID_W + GRID_W)
        cos_t[block] = jnp.where(lane < 64, jnp.broadcast_to(row_cos[i : i + 1], (64, 128)), col_cos)
        sin_t[block] = jnp.where(lane < 64, jnp.broadcast_to(row_sin[i : i + 1], (64, 128)), col_sin)
    gap = lax.broadcasted_iota(jnp.int32, (CHIP, WIN), 1) - lax.broadcasted_iota(
        jnp.int32, (CHIP, WIN), 0
    )
    band[...] = jnp.where((gap >= 0) & (gap <= 2 * WINDOW_REACH), 0.0, MASKED_SCORE)
    kv[1024:, :] = jnp.zeros((64, 256), BF16)
    pl.semaphore_wait(barrier, len(peers))

    sent = []

    def send(src, dst, s_sem, r_sem, k, to):
        copy = remote(src, dst, s_sem.at[k], r_sem.at[k], to)
        copy.start()
        sent.append(copy)
        return copy

    near = [(dz, dy) for dz in (0, 1, -1, 2) for dy in range(NY) if (dz, dy) != (0, 0)]
    near_copies = []
    for k, (dz, dy) in enumerate(near):
        to = wrap(y + dy, NY)
        near_copies.append(
            send(parts.at[to], nbuf.at[k], n_send, n_recv, k, {"z": wrap(z + dz, NZ), "y": to})
        )

    def piece(chip, core, h):
        return rows.at[rows_at((chip * NC + core) * ROWS + h * 48, 48)]

    def along(chip, h, k, to):
        source = lat.at[pl.ds(h * 48, 48)] if chip is None else piece(chip, c, h)
        slot = piece(x if chip is None else chip, c, h)
        send(source, slot, a_send, a_recv, k, {"x": to})

    def across_chip(chip, h, k):
        send(piece(chip, c, h), piece(chip, c, h), p_send, p_recv, k, partner)

    def arrived(chip, h, k):
        slot = piece(chip, c, h)
        remote(slot, slot, a_send.at[k], a_recv.at[k], {"x": right}).wait_recv()

    along(None, 0, 0, right)
    along(None, 1, 1, left)
    along(None, 1, 2, right)
    along(None, 0, 3, left)
    own_slot = rows.at[rows_at(tp * ROWS, ROWS)]
    send(lat, own_slot, p_send, p_recv, 0, partner)
    send(wo, wo_mate, m_send, m_recv, 4, partner)

    side = 1 - 2 * c

    def ctx_send(block, k, to):
        slot = cr.at[c, 0, block]
        send(slot, slot, e_send, e_recv, k, {"z": to})

    def ctx_over(block, k):
        send(cr.at[c, 0, block], cr.at[c, 1, block], o_send, o_recv, k, {"y": wrap(y + 2, NY)})

    def ctx_came(block, k):
        slot = cr.at[c, 0, block]
        remote(slot, slot, e_send.at[k], e_recv.at[k], partner).wait_recv()
        send(slot, slot, f_send, f_recv, k, partner)
        ctx_over(block, k)

    def ctx_spread(block, n):
        ctx_send(block, 3 + n, wrap(z + 1, NZ))
        ctx_send(block, 7 + n, wrap(z - 1, NZ))
        ctx_send(block, 11 + n, wrap(z + 2 * side, NZ))

    ctx_send(z, 0, wrap(z + 4, NZ))
    ctx_send(z, 1, wrap(z - 4, NZ))
    ctx_spread(z, 0)
    ctx_over(z, 15)

    for copy in near_copies:
        copy.wait_recv()
    quad = parts[y]
    for k in range(len(near)):
        quad = quad + nbuf[k]
    zsrc[...] = quad

    def z_send_to(src, slot, d):
        return send(src, zbuf.at[slot], z_send, z_recv, slot, {"z": wrap(z + d, NZ)})

    low = z_send_to(zsrc, 0, 4)
    high = z_send_to(zsrc, 1, -4)
    ctx_came(wrap(z - 1, NZ), 3)
    ctx_came(wrap(z + 1, NZ), 7)
    ctx_came(wrap(z - 2 * side, NZ), 11)
    low.wait_recv()
    far = z_send_to(zbuf.at[0], 2, 4)
    high.wait_recv()
    ctx_came(wrap(z - 4, NZ), 0)
    ctx_came(wrap(z + 4, NZ), 1)
    ctx_send(wrap(z - 4 * side, NZ), 2, wrap(z + 4 * side, NZ))
    ctx_spread(wrap(z - 4, NZ), 1)
    ctx_spread(wrap(z + 4, NZ), 2)
    arrived(left, 0, 0)
    along(left, 0, 4, right)
    across_chip(left, 0, 1)
    arrived(right, 1, 1)
    along(right, 1, 5, left)
    across_chip(right, 1, 2)
    far.wait_recv()
    total = zsrc[...] + zbuf[0] + zbuf[1] + zbuf[2]
    gsrc[...] = total
    gbuf[tp, y] = total
    g_copies = [
        send(gsrc, gbuf.at[tp, y], g_send, g_recv, k, plane_peer(*p)) for k, p in enumerate(PLANE)
    ]
    arrived(left, 1, 2)
    across_chip(left, 1, 3)
    arrived(right, 0, 3)
    across_chip(right, 0, 4)
    ctx_came(wrap(z + 8, NZ), 2)
    ctx_spread(wrap(z + 8, NZ), 3)
    for n in range(1, 4):
        step = (0, -4, 4, 8)[n]
        ctx_came(wrap(z - 1 + step, NZ), 3 + n)
        ctx_came(wrap(z + 1 + step, NZ), 7 + n)
        ctx_came(wrap(z - 2 * side + step, NZ), 11 + n)
    arrived(across, 0, 4)
    across_chip(across, 0, 5)
    arrived(across, 1, 5)
    across_chip(across, 1, 6)
    for k in range(16):
        slot = cr.at[c, 1, z]
        remote(slot, slot, o_send.at[k], o_recv.at[k], partner).wait_recv()
    send(cr.at[c, 1], cr.at[c, 1], f_send, f_recv, 15, partner)
    for copy in g_copies:
        copy.wait_recv()
    for owner in range(NTP):
        for t in range(2):
            cols = pl.ds((owner * 2 + t) * 128, 128)
            mod[0:4, cols] = gbuf[owner, t]
            mod[4:8, cols] = gbuf[owner, 2 + t]
    amp[...] = gain[...] * (1.0 + mod[1:2, :])
    camp[...] = gain[...] * (1.0 + mod[5:6, :])

    for k in range(15):
        slot = cr.at[1 - c, 0, z]
        remote(slot, slot, f_send.at[k], f_recv.at[k], partner).wait_recv()

    def normed(load, store, gains, shifts):
        acc = jnp.zeros((16, 128), F32)
        for j in range(WIDTH // 128):
            v = load(j).astype(F32)
            acc = acc + v * v
        mean = jnp.sum(acc, axis=1, keepdims=True) * (1.0 / WIDTH)
        inverse = jnp.broadcast_to(lax.rsqrt(mean + NORM_EPS), (16, 128))
        for j in range(WIDTH // 128):
            cols = slice(j * 128, j * 128 + 128)
            v = load(j).astype(F32)
            store(cols, (v * inverse * gains[:, cols] + shifts[:, cols]).astype(BF16))

    def ctx_project(column):
        def ctx_step(i, carry):
            for g in range(4):
                block = i * 4 + g
                dst = rows_at(block * CTX_ROWS, CTX_ROWS)

                def load(j):
                    return cr[j // 8, column, block, :, (j % 8) * 128 : (j % 8) * 128 + 128]

                def store(cols, value):
                    chid[dst, cols] = value

                normed(load, store, camp, mod[4:5, :])
            return carry

        lax.fori_loop(0, NZ // 4, ctx_step, 0)
        ctxkv[column] = jnp.dot(
            chid[...], wqkv[:, 256:512], preferred_element_type=F32
        ).astype(BF16)

    ctx_project(0)
    ctx_up = send(ctxkv.at[0], ctxkv.at[2], d_send, d_recv, 0, {"y": up})
    ctx_down = send(ctxkv.at[0], ctxkv.at[3], d_send, d_recv, 1, {"y": down})
    whole = cr.at[1 - c, 1]
    remote(whole, whole, f_send.at[15], f_recv.at[15], partner).wait_recv()

    remote(lat, rows.at[rows_at((x * NC + 1 - c) * ROWS, ROWS)], p_send.at[0], p_recv.at[0], partner).wait_recv()
    for chip, h, k in [(left, 0, 1), (right, 1, 2), (left, 1, 3), (right, 0, 4), (across, 0, 5), (across, 1, 6)]:
        slot = piece(chip, 1 - c, h)
        remote(slot, slot, p_send.at[k], p_recv.at[k], partner).wait_recv()

    lanes = lax.broadcasted_iota(jnp.int32, (16, 128), 1)
    first = lanes % 64 < 32

    def project(chips):
        for n, chip in enumerate(chips):
            def norm_step(i, carry):
                for g in range(4):
                    src = rows_at(chip * CHIP + i * 64 + g * 16, 16)
                    dst = rows_at(n * CHIP + i * 64 + g * 16, 16)

                    def load(j):
                        return rows[src, j * 128 : j * 128 + 128]

                    def store(cols, value):
                        hid[dst, cols] = value

                    normed(load, store, amp, mod[0:1, :])
                return carry

            lax.fori_loop(0, CHIP // 64, norm_step, 0)
        qkv[...] = jnp.dot(hid[...], wqkv[...], preferred_element_type=F32)
        for n, chip in enumerate(chips):
            def turn_step(i, carry):
                for g in range(2):
                    at = rows_at(n * CHIP + i * 32 + g * 16, 16)
                    to = rows_at(chip * CHIP + i * 32 + g * 16, 16)
                    pad = rows_at(chip * CHIP + i * 32 + g * 16 + WINDOW_REACH, 16)
                    cosine, sine = cos_t[to], sin_t[to]
                    for h in range(3):
                        u = qkv[at, h * 128 : h * 128 + 128]
                        swapped = jnp.where(first, pltpu.roll(u, 96, 1), pltpu.roll(u, 32, 1))
                        turned = (u * cosine + swapped * sine).astype(BF16)
                        if h < 2:
                            q[to, h * 128 : h * 128 + 128] = turned
                        else:
                            kv[pad, 0:128] = turned
                    kv[pad, 128:256] = qkv[at, 384:512].astype(BF16)
                return carry

            lax.fori_loop(0, CHIP // 32, turn_step, 0)

    project((0, 3))
    halo = [
        send(kv.at[pl.ds(GROUP, 128)], kv.at[pl.ds(0, 128)], h_send, h_recv, 0, after),
        send(kv.at[pl.ds(128, 128)], kv.at[pl.ds(GROUP + 128, 128)], h_send, h_recv, 1, before),
    ]
    project((1, 2))

    ctx_project(1)
    for copy in halo:
        copy.wait_recv()
    ctx_up.wait_recv()
    ctx_down.wait_recv()

    nt = (((1,), (1,)), ((), ()))
    factor = HEAD_DIM ** (-0.5) * LOG2E
    last = sp * GROUP - WINDOW_REACH

    def attend(chip):
        begin = chip * CHIP
        window = rows_at(begin, WIN)
        key_at = last + begin + lax.broadcasted_iota(jnp.int32, (1, WIN), 1)
        edge = jnp.where((key_at >= 0) & (key_at < GROUP * NZ * NY), 0.0, MASKED_SCORE)
        keys = ctxkv[:, :, 0:128].reshape(1024, 128)
        values = ctxkv[:, :, 128:256].reshape(1024, 128)
        head = lax.broadcasted_iota(jnp.int32, (2 * ROWS, 1), 0)
        sinks = jnp.where(head < ROWS, sink[0:1, 0:1], sink[0:1, 1:2]) * LOG2E

        def part(core):
            at = rows_at(begin + core * ROWS, ROWS)
            both = jnp.concatenate([q[at, 0:128], q[at, 128:256]], axis=0)
            bias = band[rows_at(core * ROWS, ROWS)] + edge
            near = lax.dot_general(both, kv[window, 0:128], nt, preferred_element_type=F32)
            near = near * factor + jnp.concatenate([bias, bias], axis=0)
            far = lax.dot_general(both, keys, nt, preferred_element_type=F32) * factor
            top = jnp.maximum(
                jnp.maximum(jnp.max(near, axis=1, keepdims=True), jnp.max(far, axis=1, keepdims=True)),
                sinks,
            )
            near = jnp.exp2(near - top)
            far = jnp.exp2(far - top)
            bottom = (
                jnp.sum(near, axis=1, keepdims=True)
                + jnp.sum(far, axis=1, keepdims=True)
                + jnp.exp2(sinks - top)
            )
            mixed = jnp.dot(near.astype(BF16), kv[window, 128:256], preferred_element_type=F32)
            mixed = mixed + jnp.dot(far.astype(BF16), values, preferred_element_type=F32)
            mixed = (mixed / bottom).astype(BF16)
            for h in range(2):
                att[chip, core, :, h * 128 : h * 128 + 128] = mixed[h * ROWS : h * ROWS + ROWS]

        part(1 - c)
        copy = send(att.at[chip, 1 - c], att_mate.at[chip], m_send, m_recv, chip, partner)
        part(c)
        return copy

    def product(chip, h):
        cols = slice(h * 1024, h * 1024 + 1024)
        return jnp.dot(att[chip, c], wo[:, cols], preferred_element_type=F32) + jnp.dot(
            att_mate[chip], wo_mate[:, cols], preferred_element_type=F32
        )

    def around(src, dst, k, to):
        return send(src, dst, s_send, s_recv, k, {"x": to})

    remote(wo, wo_mate, m_send.at[4], m_recv.at[4], partner).wait_recv()
    attend(across).wait_recv()
    opp_src[0] = product(across, 0).astype(BF16)
    first_left = around(opp_src.at[0], opp_left, 0, right)
    opp_src[1] = product(across, 1).astype(BF16)
    first_right = around(opp_src.at[1], opp_right, 1, left)
    right_mate = attend(right)
    left_mate = attend(left)
    right_mate.wait_recv()
    right_src[1] = product(right, 1).astype(BF16)
    r1 = around(right_src.at[1], from_left.at[1], 2, right)
    left_mate.wait_recv()
    left_src[0] = product(left, 0).astype(BF16)
    l0 = around(left_src.at[0], from_right.at[0], 3, left)
    own_mate = attend(x)
    right_part = product(right, 0)
    first_left.wait_recv()
    right_src[0] = (right_part + opp_left[...].astype(F32)).astype(BF16)
    r0 = around(right_src.at[0], from_left.at[0], 4, right)
    left_part = product(left, 1)
    first_right.wait_recv()
    left_src[1] = (left_part + opp_right[...].astype(F32)).astype(BF16)
    l1 = around(left_src.at[1], from_right.at[1], 5, left)
    own_mate.wait_recv()
    totals = [product(x, h) for h in range(2)]
    for copy in (r1, l0, r0, l1):
        copy.wait_recv()
    for h in range(2):
        cols = slice(h * 1024, h * 1024 + 1024)
        total = totals[h] + from_left[h].astype(F32) + from_right[h].astype(F32)
        out_ref[:, cols] = (lat[:, cols].astype(F32) + mod[2:3, cols] * total).astype(BF16)
    for copy in sent:
        copy.wait_send()


def shards(
    latent,
    condition,
    context_condition,
    context,
    norm_gain,
    shift_weight,
    scale_weight,
    gate_weight,
    query_weight,
    key_matrix,
    value_matrix,
    sink_logit_head,
    out_weight,
):
    lanes = np.arange(HEAD_DIM) % 32
    freq = (10000.0 ** (-(2.0 * lanes) / 64.0)).astype(np.float32)[None]
    vm = pltpu.VMEM
    dma = pltpu.SemaphoreType.DMA
    half = (2, ROWS, WIDTH // 2)
    return pl.pallas_call(
        block_kernel,
        out_shape=jax.ShapeDtypeStruct((ROWS, WIDTH), BF16),
        in_specs=[pl.BlockSpec(memory_space=pl.ANY)] * 14,
        out_specs=pl.BlockSpec(memory_space=pltpu.VMEM),
        scratch_shapes=[
            vm((ROWS, WIDTH), BF16), vm((2, 2, NZ, CTX_ROWS, WIDTH // 2), BF16), vm((1, WIDTH), F32),
            vm((1, 32), F32), vm((1, 32), F32),
            vm((32, 256), BF16), vm((32, 256), BF16), vm((32, 256), BF16),
            vm((WIDTH, 512), BF16), vm((1, 2), F32), vm((256, WIDTH), BF16), vm((1, 128), F32),
            vm((GROUP, WIDTH), BF16),
            vm((4, 4, 128), F32), vm((15, 4, 128), F32), vm((4, 128), F32), vm((3, 4, 128), F32),
            vm((4, 128), F32), vm((NTP, NY, 4, 128), F32),
            vm((8, WIDTH), F32), vm((1, WIDTH), F32), vm((1, WIDTH), F32),
            vm((GROUP, 128), F32), vm((GROUP, 128), F32), vm((CHIP, WIN), F32),
            vm((2 * CHIP, WIDTH), BF16), vm((NZ * CTX_ROWS, WIDTH), BF16), vm((2 * CHIP, 512), F32),
            vm((GROUP, 256), BF16), vm((GROUP + 256 + 64, 256), BF16),
            vm((NY, NZ * CTX_ROWS, 256), BF16),
            vm((NX, NC, ROWS, 256), BF16), vm((NX, ROWS, 256), BF16), vm((256, WIDTH), BF16),
            vm(half, BF16), vm(half, BF16), vm(half, BF16),
            vm(half[1:], BF16), vm(half[1:], BF16), vm(half, BF16), vm(half, BF16),
            dma((16,)),
            dma((15,)), dma((15,)), dma((3,)), dma((3,)), dma((31,)), dma((31,)),
            dma((6,)), dma((6,)), dma((7,)), dma((7,)),
            dma((15,)), dma((15,)), dma((16,)), dma((16,)), dma((16,)), dma((16,)), dma((2,)), dma((2,)), dma((2,)), dma((2,)),
            dma((5,)), dma((5,)), dma((6,)), dma((6,)),
        ],
        compiler_params=pltpu.CompilerParams(
            collective_id=0, has_side_effects=True, vmem_limit_bytes=62 * 1024 * 1024
        ),
        cost_estimate=pl.CostEstimate(flops=10**9, bytes_accessed=10**7, transcendentals=0),
        name="block",
    )(
        latent, context, norm_gain.reshape(1, -1), condition.reshape(1, -1),
        context_condition.reshape(1, -1), shift_weight, scale_weight, gate_weight,
        query_weight, key_matrix, value_matrix, sink_logit_head.reshape(1, -1), out_weight,
        jnp.asarray(freq),
    )


def solution(mesh):
    torus = Mesh(mesh.devices.reshape(NZ, NY, NX, NC), ALL)
    return jax.shard_map(
        shards,
        mesh=torus,
        in_specs=(
            P(ALL, None),
            P(SP),
            P(SP),
            P(SP, None),
            P(),
            P(SP, TP),
            P(SP, TP),
            P(SP, TP),
            P(None, TP),
            P(None, TP),
            P(None, TP),
            P(TP),
            P(TP, None),
        ),
        out_specs=P(ALL, None),
        check_vma=False,
    )
```

```python
import functools

import jax
import jax.numpy as jnp
import numpy as np
from jax import lax
from jax.experimental import pallas as pl
from jax.experimental.pallas import tpu as pltpu
from jax.sharding import Mesh
from jax.sharding import PartitionSpec as P

HEAD_DIM = 128
WINDOW_REACH = 128
GRID_W = 64
SP = ("z", "y")
TP = ("x", "c")
ALL = ("z", "y", "x", "c")
MESH = pl.DeviceIdType.MESH

NORM_EPS = 1e-05
MASKED_SCORE = -1e30
LOG2E = 1.4426950408889634
NZ, NY, NX, NC = 16, 4, 4, 2
NTP = NX * NC
WIDTH = 2048
ROWS = 96
GROUP = ROWS * NTP
CHIP = ROWS * NC
CTX_ROWS = 16
WIN = 512
F32 = jnp.float32
BF16 = jnp.bfloat16
PLANE = [
    (dy, dx, dc)
    for dy in (2, 1, 3, 0)
    for dx in (2, 1, 3, 0)
    for dc in (1, 0)
    if (dy, dx, dc) != (0, 0, 0)
]


def wrap(value, size):
    return lax.rem(value + size, size)


def remote(src, dst, send, recv, device):
    return pltpu.make_async_remote_copy(
        src_ref=src,
        dst_ref=dst,
        send_sem=send,
        recv_sem=recv,
        device_id=device,
        device_id_type=MESH,
    )


def rows_at(start, count):
    return pl.ds(pl.multiple_of(start, 16), count)


def block_kernel(
    lat_hbm, ctx_hbm, gain_hbm, cond_hbm, cctx_hbm, sw_hbm, cw_hbm, gw_hbm,
    wq_hbm, wk_hbm, wv_hbm, sink_hbm, wo_hbm, freq_hbm,
    out_ref,
    lat, cr, gain, cond, cctx, sw, cw, gw, wqkv, sink, wo, freq,
    rows, parts, nbuf, zsrc, zbuf, gsrc, gbuf, mod, amp, camp,
    cos_t, sin_t, band, hid, chid, qkv, q, kv, ctxkv,
    att, att_mate, wo_mate, opp_src, right_src, left_src, opp_left, opp_right, from_left, from_right,
    l_sem, n_send, n_recv, z_send, z_recv, g_send, g_recv, a_send, a_recv, p_send, p_recv,
    e_send, e_recv, f_send, f_recv, o_send, o_recv, d_send, d_recv, h_send, h_recv, m_send, m_recv, s_send, s_recv,
):
    z, y, x, c = (lax.axis_index(a) for a in ALL)
    tp = x * NC + c
    sp = z * NY + y
    right, left, across = wrap(x + 1, NX), wrap(x - 1, NX), wrap(x + 2, NX)
    up, down = wrap(y + 1, NY), wrap(y - 1, NY)
    partner = {"c": 1 - c}
    after = {"z": wrap(z + (y + 1) // NY, NZ), "y": up}
    before = {"z": wrap(z - (NY - y) // NY, NZ), "y": down}

    def plane_peer(dy, dx, dc):
        return {"y": wrap(y + dy, NY), "x": wrap(x + dx, NX), "c": wrap(c + dc, NC)}

    barrier = pltpu.get_barrier_semaphore()
    peers = [{"z": wrap(z + d, NZ)} for d in (1, -1, 2, -2, 4, -4)]
    peers += [
        {"z": wrap(z + d, NZ), "y": wrap(y + e, NY)} for d in (1, -1, 2, -2) for e in range(1, NY)
    ]
    peers += [plane_peer(*p) for p in PLANE] + [after, before]
    for peer in peers:
        pl.semaphore_signal(barrier, inc=1, device_id=peer, device_id_type=MESH)
    pairs = [
        (cond_hbm, cond), (cctx_hbm, cctx), (sw_hbm, sw), (cw_hbm, cw), (gw_hbm, gw),
        (lat_hbm, lat), (freq_hbm, freq), (gain_hbm, gain), (sink_hbm, sink),
        (ctx_hbm.at[:, pl.ds(0, 1024)], cr.at[0, 0, z]),
        (ctx_hbm.at[:, pl.ds(1024, 1024)], cr.at[1, 0, z]),
        (wq_hbm, wqkv.at[:, pl.ds(0, 256)]), (wk_hbm, wqkv.at[:, pl.ds(256, 128)]),
        (wv_hbm, wqkv.at[:, pl.ds(384, 128)]), (wo_hbm, wo),
        (lat_hbm, rows.at[rows_at(tp * ROWS, ROWS)]),
    ]
    local = [pltpu.make_async_copy(s, d, l_sem.at[k]) for k, (s, d) in enumerate(pairs)]
    for copy in local:
        copy.start()

    for copy in local[:5]:
        copy.wait()
    row = lax.broadcasted_iota(jnp.int32, (8, 32), 0)
    vectors = jnp.where(
        row == 0, jnp.broadcast_to(cond[...], (8, 32)), jnp.broadcast_to(cctx[...], (8, 32))
    )
    active = (vectors / (1.0 + jnp.exp(-vectors))).astype(BF16)
    shift_part = jnp.dot(active, sw[...], preferred_element_type=F32)
    scale_part = jnp.dot(active, cw[...], preferred_element_type=F32)
    gate_part = jnp.dot(active, gw[...], preferred_element_type=F32)
    for t in range(2):
        cols = slice(t * 128, t * 128 + 128)
        parts[t] = jnp.concatenate(
            [shift_part[0:1, cols], scale_part[0:1, cols], gate_part[0:1, cols], gate_part[0:1, cols]],
            axis=0,
        )
        parts[2 + t] = jnp.concatenate(
            [shift_part[1:2, cols], scale_part[1:2, cols], scale_part[1:2, cols], scale_part[1:2, cols]],
            axis=0,
        )
    for copy in local[5:]:
        copy.wait()

    lane = lax.broadcasted_iota(jnp.int32, (64, 128), 1)
    sign = jnp.where(lane % 64 < 32, -1.0, 1.0)
    col_angle = lax.broadcasted_iota(jnp.int32, (64, 128), 0).astype(F32) * freq[...]
    col_cos, col_sin = jnp.cos(col_angle), jnp.sin(col_angle) * sign
    row_ids = sp * (GROUP // GRID_W) + lax.broadcasted_iota(jnp.int32, (16, 128), 0)
    row_angle = row_ids.astype(F32) * freq[...]
    row_cos, row_sin = jnp.cos(row_angle), jnp.sin(row_angle) * sign[0:16]
    for i in range(GROUP // GRID_W):
        block = slice(i * GRID_W, i * GRID_W + GRID_W)
        cos_t[block] = jnp.where(lane < 64, jnp.broadcast_to(row_cos[i : i + 1], (64, 128)), col_cos)
        sin_t[block] = jnp.where(lane < 64, jnp.broadcast_to(row_sin[i : i + 1], (64, 128)), col_sin)
    gap = lax.broadcasted_iota(jnp.int32, (CHIP, WIN), 1) - lax.broadcasted_iota(
        jnp.int32, (CHIP, WIN), 0
    )
    band[...] = jnp.where((gap >= 0) & (gap <= 2 * WINDOW_REACH), 0.0, MASKED_SCORE)
    kv[1024:, :] = jnp.zeros((64, 256), BF16)
    pl.semaphore_wait(barrier, len(peers))

    sent = []

    def send(src, dst, s_sem, r_sem, k, to):
        copy = remote(src, dst, s_sem.at[k], r_sem.at[k], to)
        copy.start()
        sent.append(copy)
        return copy

    near = [(dz, dy) for dz in (0, 1, -1, 2) for dy in range(NY) if (dz, dy) != (0, 0)]
    near_copies = []
    for k, (dz, dy) in enumerate(near):
        to = wrap(y + dy, NY)
        near_copies.append(
            send(parts.at[to], nbuf.at[k], n_send, n_recv, k, {"z": wrap(z + dz, NZ), "y": to})
        )

    def piece(chip, core, h):
        return rows.at[rows_at((chip * NC + core) * ROWS + h * 48, 48)]

    def along(chip, h, k, to):
        source = lat.at[pl.ds(h * 48, 48)] if chip is None else piece(chip, c, h)
        slot = piece(x if chip is None else chip, c, h)
        send(source, slot, a_send, a_recv, k, {"x": to})

    def across_chip(chip, h, k):
        send(piece(chip, c, h), piece(chip, c, h), p_send, p_recv, k, partner)

    def arrived(chip, h, k):
        slot = piece(chip, c, h)
        remote(slot, slot, a_send.at[k], a_recv.at[k], {"x": right}).wait_recv()

    along(None, 0, 0, right)
    along(None, 1, 1, left)
    along(None, 1, 2, right)
    along(None, 0, 3, left)
    own_slot = rows.at[rows_at(tp * ROWS, ROWS)]
    send(lat, own_slot, p_send, p_recv, 0, partner)
    send(wo, wo_mate, m_send, m_recv, 4, partner)

    side = 1 - 2 * c

    def ctx_send(block, k, to):
        slot = cr.at[c, 0, block]
        send(slot, slot, e_send, e_recv, k, {"z": to})

    def ctx_over(block, k):
        send(cr.at[c, 0, block], cr.at[c, 1, block], o_send, o_recv, k, {"y": wrap(y + 2, NY)})

    def ctx_came(block, k):
        slot = cr.at[c, 0, block]
        remote(slot, slot, e_send.at[k], e_recv.at[k], partner).wait_recv()
        send(slot, slot, f_send, f_recv, k, partner)
        ctx_over(block, k)

    def ctx_spread(block, n):
        ctx_send(block, 3 + n, wrap(z + 1, NZ))
        ctx_send(block, 7 + n, wrap(z - 1, NZ))
        ctx_send(block, 11 + n, wrap(z + 2 * side, NZ))

    ctx_send(z, 0, wrap(z + 4, NZ))
    ctx_send(z, 1, wrap(z - 4, NZ))
    ctx_spread(z, 0)
    ctx_over(z, 15)

    for copy in near_copies:
        copy.wait_recv()
    quad = parts[y]
    for k in range(len(near)):
        quad = quad + nbuf[k]
    zsrc[...] = quad

    def z_send_to(src, slot, d):
        return send(src, zbuf.at[slot], z_send, z_recv, slot, {"z": wrap(z + d, NZ)})

    low = z_send_to(zsrc, 0, 4)
    high = z_send_to(zsrc, 1, -4)
    ctx_came(wrap(z - 1, NZ), 3)
    ctx_came(wrap(z + 1, NZ), 7)
    ctx_came(wrap(z - 2 * side, NZ), 11)
    low.wait_recv()
    far = z_send_to(zbuf.at[0], 2, 4)
    high.wait_recv()
    ctx_came(wrap(z - 4, NZ), 0)
    ctx_came(wrap(z + 4, NZ), 1)
    ctx_send(wrap(z - 4 * side, NZ), 2, wrap(z + 4 * side, NZ))
    ctx_spread(wrap(z - 4, NZ), 1)
    ctx_spread(wrap(z + 4, NZ), 2)
    arrived(left, 0, 0)
    along(left, 0, 4, right)
    across_chip(left, 0, 1)
    arrived(right, 1, 1)
    along(right, 1, 5, left)
    across_chip(right, 1, 2)
    far.wait_recv()
    total = zsrc[...] + zbuf[0] + zbuf[1] + zbuf[2]
    gsrc[...] = total
    gbuf[tp, y] = total
    g_copies = [
        send(gsrc, gbuf.at[tp, y], g_send, g_recv, k, plane_peer(*p)) for k, p in enumerate(PLANE)
    ]
    arrived(left, 1, 2)
    across_chip(left, 1, 3)
    arrived(right, 0, 3)
    across_chip(right, 0, 4)
    ctx_came(wrap(z + 8, NZ), 2)
    ctx_spread(wrap(z + 8, NZ), 3)
    for n in range(1, 4):
        step = (0, -4, 4, 8)[n]
        ctx_came(wrap(z - 1 + step, NZ), 3 + n)
        ctx_came(wrap(z + 1 + step, NZ), 7 + n)
        ctx_came(wrap(z - 2 * side + step, NZ), 11 + n)
    arrived(across, 0, 4)
    across_chip(across, 0, 5)
    arrived(across, 1, 5)
    across_chip(across, 1, 6)
    for copy in g_copies:
        copy.wait_recv()
    for owner in range(NTP):
        for t in range(2):
            cols = pl.ds((owner * 2 + t) * 128, 128)
            mod[0:4, cols] = gbuf[owner, t]
            mod[4:8, cols] = gbuf[owner, 2 + t]
    amp[...] = gain[...] * (1.0 + mod[1:2, :])
    camp[...] = gain[...] * (1.0 + mod[5:6, :])

    for k in range(15):
        slot = cr.at[1 - c, 0, z]
        remote(slot, slot, f_send.at[k], f_recv.at[k], partner).wait_recv()

    def normed(load, store, gains, shifts):
        acc = jnp.zeros((16, 128), F32)
        for j in range(WIDTH // 128):
            v = load(j).astype(F32)
            acc = acc + v * v
        mean = jnp.sum(acc, axis=1, keepdims=True) * (1.0 / WIDTH)
        inverse = jnp.broadcast_to(lax.rsqrt(mean + NORM_EPS), (16, 128))
        for j in range(WIDTH // 128):
            cols = slice(j * 128, j * 128 + 128)
            v = load(j).astype(F32)
            store(cols, (v * inverse * gains[:, cols] + shifts[:, cols]).astype(BF16))

    def ctx_project(column):
        def ctx_step(i, carry):
            for g in range(4):
                block = i * 4 + g
                dst = rows_at(block * CTX_ROWS, CTX_ROWS)

                def load(j):
                    return cr[j // 8, column, block, :, (j % 8) * 128 : (j % 8) * 128 + 128]

                def store(cols, value):
                    chid[dst, cols] = value

                normed(load, store, camp, mod[4:5, :])
            return carry

        lax.fori_loop(0, NZ // 4, ctx_step, 0)
        ctxkv[column] = jnp.dot(
            chid[...], wqkv[:, 256:512], preferred_element_type=F32
        ).astype(BF16)

    ctx_project(0)
    ctx_up = send(ctxkv.at[0], ctxkv.at[2], d_send, d_recv, 0, {"y": up})
    ctx_down = send(ctxkv.at[0], ctxkv.at[3], d_send, d_recv, 1, {"y": down})

    remote(lat, rows.at[rows_at((x * NC + 1 - c) * ROWS, ROWS)], p_send.at[0], p_recv.at[0], partner).wait_recv()
    for chip, h, k in [(left, 0, 1), (right, 1, 2), (left, 1, 3), (right, 0, 4), (across, 0, 5), (across, 1, 6)]:
        slot = piece(chip, 1 - c, h)
        remote(slot, slot, p_send.at[k], p_recv.at[k], partner).wait_recv()

    lanes = lax.broadcasted_iota(jnp.int32, (16, 128), 1)
    first = lanes % 64 < 32

    def project(chips):
        for n, chip in enumerate(chips):
            def norm_step(i, carry):
                for g in range(4):
                    src = rows_at(chip * CHIP + i * 64 + g * 16, 16)
                    dst = rows_at(n * CHIP + i * 64 + g * 16, 16)

                    def load(j):
                        return rows[src, j * 128 : j * 128 + 128]

                    def store(cols, value):
                        hid[dst, cols] = value

                    normed(load, store, amp, mod[0:1, :])
                return carry

            lax.fori_loop(0, CHIP // 64, norm_step, 0)
        qkv[...] = jnp.dot(hid[...], wqkv[...], preferred_element_type=F32)
        for n, chip in enumerate(chips):
            def turn_step(i, carry):
                for g in range(2):
                    at = rows_at(n * CHIP + i * 32 + g * 16, 16)
                    to = rows_at(chip * CHIP + i * 32 + g * 16, 16)
                    pad = rows_at(chip * CHIP + i * 32 + g * 16 + WINDOW_REACH, 16)
                    cosine, sine = cos_t[to], sin_t[to]
                    for h in range(3):
                        u = qkv[at, h * 128 : h * 128 + 128]
                        swapped = jnp.where(first, pltpu.roll(u, 96, 1), pltpu.roll(u, 32, 1))
                        turned = (u * cosine + swapped * sine).astype(BF16)
                        if h < 2:
                            q[to, h * 128 : h * 128 + 128] = turned
                        else:
                            kv[pad, 0:128] = turned
                    kv[pad, 128:256] = qkv[at, 384:512].astype(BF16)
                return carry

            lax.fori_loop(0, CHIP // 32, turn_step, 0)

    project((0, 3))
    halo = [
        send(kv.at[pl.ds(GROUP, 128)], kv.at[pl.ds(0, 128)], h_send, h_recv, 0, after),
        send(kv.at[pl.ds(128, 128)], kv.at[pl.ds(GROUP + 128, 128)], h_send, h_recv, 1, before),
    ]
    for k in range(16):
        slot = cr.at[c, 1, z]
        remote(slot, slot, o_send.at[k], o_recv.at[k], partner).wait_recv()
    send(cr.at[c, 1], cr.at[c, 1], f_send, f_recv, 15, partner)
    project((1, 2))
    whole = cr.at[1 - c, 1]
    remote(whole, whole, f_send.at[15], f_recv.at[15], partner).wait_recv()

    ctx_project(1)
    for copy in halo:
        copy.wait_recv()
    ctx_up.wait_recv()
    ctx_down.wait_recv()

    nt = (((1,), (1,)), ((), ()))
    factor = HEAD_DIM ** (-0.5) * LOG2E
    last = sp * GROUP - WINDOW_REACH

    def attend(chip):
        begin = chip * CHIP
        window = rows_at(begin, WIN)
        key_at = last + begin + lax.broadcasted_iota(jnp.int32, (1, WIN), 1)
        edge = jnp.where((key_at >= 0) & (key_at < GROUP * NZ * NY), 0.0, MASKED_SCORE)
        keys = ctxkv[:, :, 0:128].reshape(1024, 128)
        values = ctxkv[:, :, 128:256].reshape(1024, 128)
        head = lax.broadcasted_iota(jnp.int32, (2 * ROWS, 1), 0)
        sinks = jnp.where(head < ROWS, sink[0:1, 0:1], sink[0:1, 1:2]) * LOG2E

        def part(core):
            at = rows_at(begin + core * ROWS, ROWS)
            both = jnp.concatenate([q[at, 0:128], q[at, 128:256]], axis=0)
            bias = band[rows_at(core * ROWS, ROWS)] + edge
            near = lax.dot_general(both, kv[window, 0:128], nt, preferred_element_type=F32)
            near = near * factor + jnp.concatenate([bias, bias], axis=0)
            far = lax.dot_general(both, keys, nt, preferred_element_type=F32) * factor
            top = jnp.maximum(
                jnp.maximum(jnp.max(near, axis=1, keepdims=True), jnp.max(far, axis=1, keepdims=True)),
                sinks,
            )
            near = jnp.exp2(near - top)
            far = jnp.exp2(far - top)
            bottom = (
                jnp.sum(near, axis=1, keepdims=True)
                + jnp.sum(far, axis=1, keepdims=True)
                + jnp.exp2(sinks - top)
            )
            mixed = jnp.dot(near.astype(BF16), kv[window, 128:256], preferred_element_type=F32)
            mixed = mixed + jnp.dot(far.astype(BF16), values, preferred_element_type=F32)
            mixed = (mixed / bottom).astype(BF16)
            for h in range(2):
                att[chip, core, :, h * 128 : h * 128 + 128] = mixed[h * ROWS : h * ROWS + ROWS]

        part(1 - c)
        copy = send(att.at[chip, 1 - c], att_mate.at[chip], m_send, m_recv, chip, partner)
        part(c)
        return copy

    def product(chip, h):
        cols = slice(h * 1024, h * 1024 + 1024)
        return jnp.dot(att[chip, c], wo[:, cols], preferred_element_type=F32) + jnp.dot(
            att_mate[chip], wo_mate[:, cols], preferred_element_type=F32
        )

    def around(src, dst, k, to):
        return send(src, dst, s_send, s_recv, k, {"x": to})

    remote(wo, wo_mate, m_send.at[4], m_recv.at[4], partner).wait_recv()
    attend(across).wait_recv()
    opp_src[0] = product(across, 0).astype(BF16)
    first_left = around(opp_src.at[0], opp_left, 0, right)
    opp_src[1] = product(across, 1).astype(BF16)
    first_right = around(opp_src.at[1], opp_right, 1, left)
    right_mate = attend(right)
    left_mate = attend(left)
    right_mate.wait_recv()
    right_src[1] = product(right, 1).astype(BF16)
    r1 = around(right_src.at[1], from_left.at[1], 2, right)
    left_mate.wait_recv()
    left_src[0] = product(left, 0).astype(BF16)
    l0 = around(left_src.at[0], from_right.at[0], 3, left)
    own_mate = attend(x)
    right_part = product(right, 0)
    first_left.wait_recv()
    right_src[0] = (right_part + opp_left[...].astype(F32)).astype(BF16)
    r0 = around(right_src.at[0], from_left.at[0], 4, right)
    left_part = product(left, 1)
    first_right.wait_recv()
    left_src[1] = (left_part + opp_right[...].astype(F32)).astype(BF16)
    l1 = around(left_src.at[1], from_right.at[1], 5, left)
    own_mate.wait_recv()
    totals = [product(x, h) for h in range(2)]
    for copy in (r1, l0, r0, l1):
        copy.wait_recv()
    for h in range(2):
        cols = slice(h * 1024, h * 1024 + 1024)
        total = totals[h] + from_left[h].astype(F32) + from_right[h].astype(F32)
        out_ref[:, cols] = (lat[:, cols].astype(F32) + mod[2:3, cols] * total).astype(BF16)
    for copy in sent:
        copy.wait_send()


def shards(
    latent,
    condition,
    context_condition,
    context,
    norm_gain,
    shift_weight,
    scale_weight,
    gate_weight,
    query_weight,
    key_matrix,
    value_matrix,
    sink_logit_head,
    out_weight,
):
    lanes = np.arange(HEAD_DIM) % 32
    freq = (10000.0 ** (-(2.0 * lanes) / 64.0)).astype(np.float32)[None]
    vm = pltpu.VMEM
    dma = pltpu.SemaphoreType.DMA
    half = (2, ROWS, WIDTH // 2)
    return pl.pallas_call(
        block_kernel,
        out_shape=jax.ShapeDtypeStruct((ROWS, WIDTH), BF16),
        in_specs=[pl.BlockSpec(memory_space=pl.ANY)] * 14,
        out_specs=pl.BlockSpec(memory_space=pltpu.VMEM),
        scratch_shapes=[
            vm((ROWS, WIDTH), BF16), vm((2, 2, NZ, CTX_ROWS, WIDTH // 2), BF16), vm((1, WIDTH), F32),
            vm((1, 32), F32), vm((1, 32), F32),
            vm((32, 256), BF16), vm((32, 256), BF16), vm((32, 256), BF16),
            vm((WIDTH, 512), BF16), vm((1, 2), F32), vm((256, WIDTH), BF16), vm((1, 128), F32),
            vm((GROUP, WIDTH), BF16),
            vm((4, 4, 128), F32), vm((15, 4, 128), F32), vm((4, 128), F32), vm((3, 4, 128), F32),
            vm((4, 128), F32), vm((NTP, NY, 4, 128), F32),
            vm((8, WIDTH), F32), vm((1, WIDTH), F32), vm((1, WIDTH), F32),
            vm((GROUP, 128), F32), vm((GROUP, 128), F32), vm((CHIP, WIN), F32),
            vm((2 * CHIP, WIDTH), BF16), vm((NZ * CTX_ROWS, WIDTH), BF16), vm((2 * CHIP, 512), F32),
            vm((GROUP, 256), BF16), vm((GROUP + 256 + 64, 256), BF16),
            vm((NY, NZ * CTX_ROWS, 256), BF16),
            vm((NX, NC, ROWS, 256), BF16), vm((NX, ROWS, 256), BF16), vm((256, WIDTH), BF16),
            vm(half, BF16), vm(half, BF16), vm(half, BF16),
            vm(half[1:], BF16), vm(half[1:], BF16), vm(half, BF16), vm(half, BF16),
            dma((16,)),
            dma((15,)), dma((15,)), dma((3,)), dma((3,)), dma((31,)), dma((31,)),
            dma((6,)), dma((6,)), dma((7,)), dma((7,)),
            dma((15,)), dma((15,)), dma((16,)), dma((16,)), dma((16,)), dma((16,)), dma((2,)), dma((2,)), dma((2,)), dma((2,)),
            dma((5,)), dma((5,)), dma((6,)), dma((6,)),
        ],
        compiler_params=pltpu.CompilerParams(
            collective_id=0, has_side_effects=True, vmem_limit_bytes=62 * 1024 * 1024
        ),
        cost_estimate=pl.CostEstimate(flops=10**9, bytes_accessed=10**7, transcendentals=0),
        name="block",
    )(
        latent, context, norm_gain.reshape(1, -1), condition.reshape(1, -1),
        context_condition.reshape(1, -1), shift_weight, scale_weight, gate_weight,
        query_weight, key_matrix, value_matrix, sink_logit_head.reshape(1, -1), out_weight,
        jnp.asarray(freq),
    )


def solution(mesh):
    torus = Mesh(mesh.devices.reshape(NZ, NY, NX, NC), ALL)
    return jax.shard_map(
        shards,
        mesh=torus,
        in_specs=(
            P(ALL, None),
            P(SP),
            P(SP),
            P(SP, None),
            P(),
            P(SP, TP),
            P(SP, TP),
            P(SP, TP),
            P(None, TP),
            P(None, TP),
            P(None, TP),
            P(TP),
            P(TP, None),
        ),
        out_specs=P(ALL, None),
        check_vma=False,
    )
```

```python
import functools

import jax
import jax.numpy as jnp
import numpy as np
from jax import lax
from jax.experimental import pallas as pl
from jax.experimental.pallas import tpu as pltpu
from jax.sharding import Mesh
from jax.sharding import PartitionSpec as P

HEAD_DIM = 128
WINDOW_REACH = 128
GRID_W = 64
SP = ("z", "y")
TP = ("x", "c")
ALL = ("z", "y", "x", "c")
MESH = pl.DeviceIdType.MESH

NORM_EPS = 1e-05
MASKED_SCORE = -1e30
LOG2E = 1.4426950408889634
NZ, NY, NX, NC = 16, 4, 4, 2
NTP = NX * NC
WIDTH = 2048
ROWS = 96
GROUP = ROWS * NTP
CHIP = ROWS * NC
CTX_ROWS = 16
WIN = 512
F32 = jnp.float32
BF16 = jnp.bfloat16
PLANE = [
    (dy, dx, dc)
    for dy in (2, 1, 3, 0)
    for dx in (2, 1, 3, 0)
    for dc in (1, 0)
    if (dy, dx, dc) != (0, 0, 0)
]


def wrap(value, size):
    return lax.rem(value + size, size)


def remote(src, dst, send, recv, device):
    return pltpu.make_async_remote_copy(
        src_ref=src,
        dst_ref=dst,
        send_sem=send,
        recv_sem=recv,
        device_id=device,
        device_id_type=MESH,
    )


def rows_at(start, count):
    return pl.ds(pl.multiple_of(start, 16), count)


def block_kernel(
    lat_hbm, ctx_hbm, gain_hbm, cond_hbm, cctx_hbm, sw_hbm, cw_hbm, gw_hbm,
    wq_hbm, wk_hbm, wv_hbm, sink_hbm, wo_hbm, freq_hbm,
    out_ref,
    lat, cr, gain, cond, cctx, sw, cw, gw, wqkv, sink, wo, freq,
    rows, parts, nbuf, zsrc, zbuf, gsrc, gbuf, mod, amp, camp, shift, cshift,
    cos_t, sin_t, band, hid, chid, qkv, q, kv, ctxkv,
    att, att_mate, wo_mate, opp_src, right_src, left_src, opp_left, opp_right, from_left, from_right,
    l_sem, n_send, n_recv, z_send, z_recv, g_send, g_recv, a_send, a_recv, p_send, p_recv,
    e_send, e_recv, f_send, f_recv, o_send, o_recv, d_send, d_recv, h_send, h_recv, m_send, m_recv, s_send, s_recv,
):
    z, y, x, c = (lax.axis_index(a) for a in ALL)
    tp = x * NC + c
    sp = z * NY + y
    right, left, across = wrap(x + 1, NX), wrap(x - 1, NX), wrap(x + 2, NX)
    up, down = wrap(y + 1, NY), wrap(y - 1, NY)
    partner = {"c": 1 - c}
    after = {"z": wrap(z + (y + 1) // NY, NZ), "y": up}
    before = {"z": wrap(z - (NY - y) // NY, NZ), "y": down}

    def plane_peer(dy, dx, dc):
        return {"y": wrap(y + dy, NY), "x": wrap(x + dx, NX), "c": wrap(c + dc, NC)}

    barrier = pltpu.get_barrier_semaphore()
    peers = [{"z": wrap(z + d, NZ)} for d in (1, -1, 2, -2, 4, -4)]
    peers += [
        {"z": wrap(z + d, NZ), "y": wrap(y + e, NY)} for d in (1, -1, 2, -2) for e in range(1, NY)
    ]
    peers += [plane_peer(*p) for p in PLANE] + [after, before]
    for peer in peers:
        pl.semaphore_signal(barrier, inc=1, device_id=peer, device_id_type=MESH)
    pairs = [
        (cond_hbm, cond), (cctx_hbm, cctx), (sw_hbm, sw), (cw_hbm, cw), (gw_hbm, gw),
        (lat_hbm, lat), (freq_hbm, freq), (gain_hbm, gain), (sink_hbm, sink),
        (ctx_hbm.at[:, pl.ds(0, 1024)], cr.at[0, 0, z]),
        (ctx_hbm.at[:, pl.ds(1024, 1024)], cr.at[1, 0, z]),
        (wq_hbm, wqkv.at[:, pl.ds(0, 256)]), (wk_hbm, wqkv.at[:, pl.ds(256, 128)]),
        (wv_hbm, wqkv.at[:, pl.ds(384, 128)]), (wo_hbm, wo),
        (lat_hbm, rows.at[rows_at(tp * ROWS, ROWS)]),
    ]
    local = [pltpu.make_async_copy(s, d, l_sem.at[k]) for k, (s, d) in enumerate(pairs)]
    for copy in local:
        copy.start()

    for copy in local[:5]:
        copy.wait()
    row = lax.broadcasted_iota(jnp.int32, (8, 32), 0)
    vectors = jnp.where(
        row == 0, jnp.broadcast_to(cond[...], (8, 32)), jnp.broadcast_to(cctx[...], (8, 32))
    )
    active = (vectors / (1.0 + jnp.exp(-vectors))).astype(BF16)
    shift_part = jnp.dot(active, sw[...], preferred_element_type=F32)
    scale_part = jnp.dot(active, cw[...], preferred_element_type=F32)
    gate_part = jnp.dot(active, gw[...], preferred_element_type=F32)
    for t in range(2):
        cols = slice(t * 128, t * 128 + 128)
        parts[t] = jnp.concatenate(
            [shift_part[0:1, cols], scale_part[0:1, cols], gate_part[0:1, cols], gate_part[0:1, cols]],
            axis=0,
        )
        parts[2 + t] = jnp.concatenate(
            [shift_part[1:2, cols], scale_part[1:2, cols], scale_part[1:2, cols], scale_part[1:2, cols]],
            axis=0,
        )
    for copy in local[5:]:
        copy.wait()

    lane = lax.broadcasted_iota(jnp.int32, (64, 128), 1)
    sign = jnp.where(lane % 64 < 32, -1.0, 1.0)
    col_angle = lax.broadcasted_iota(jnp.int32, (64, 128), 0).astype(F32) * freq[...]
    col_cos, col_sin = jnp.cos(col_angle), jnp.sin(col_angle) * sign
    row_ids = sp * (GROUP // GRID_W) + lax.broadcasted_iota(jnp.int32, (16, 128), 0)
    row_angle = row_ids.astype(F32) * freq[...]
    row_cos, row_sin = jnp.cos(row_angle), jnp.sin(row_angle) * sign[0:16]
    for i in range(GROUP // GRID_W):
        block = slice(i * GRID_W, i * GRID_W + GRID_W)
        cos_t[block] = jnp.where(lane < 64, jnp.broadcast_to(row_cos[i : i + 1], (64, 128)), col_cos)
        sin_t[block] = jnp.where(lane < 64, jnp.broadcast_to(row_sin[i : i + 1], (64, 128)), col_sin)
    gap = lax.broadcasted_iota(jnp.int32, (CHIP, WIN), 1) - lax.broadcasted_iota(
        jnp.int32, (CHIP, WIN), 0
    )
    band[...] = jnp.where((gap >= 0) & (gap <= 2 * WINDOW_REACH), 0.0, MASKED_SCORE)
    kv[1024:, :] = jnp.zeros((64, 256), BF16)
    pl.semaphore_wait(barrier, len(peers))

    sent = []

    def send(src, dst, s_sem, r_sem, k, to):
        copy = remote(src, dst, s_sem.at[k], r_sem.at[k], to)
        copy.start()
        sent.append(copy)
        return copy

    near = [(dz, dy) for dz in (0, 1, -1, 2) for dy in range(NY) if (dz, dy) != (0, 0)]
    near_copies = []
    for k, (dz, dy) in enumerate(near):
        to = wrap(y + dy, NY)
        near_copies.append(
            send(parts.at[to], nbuf.at[k], n_send, n_recv, k, {"z": wrap(z + dz, NZ), "y": to})
        )

    def piece(chip, core, h):
        return rows.at[rows_at((chip * NC + core) * ROWS + h * 48, 48)]

    def along(chip, h, k, to):
        source = lat.at[pl.ds(h * 48, 48)] if chip is None else piece(chip, c, h)
        slot = piece(x if chip is None else chip, c, h)
        send(source, slot, a_send, a_recv, k, {"x": to})

    def across_chip(chip, h, k):
        send(piece(chip, c, h), piece(chip, c, h), p_send, p_recv, k, partner)

    def arrived(chip, h, k):
        slot = piece(chip, c, h)
        remote(slot, slot, a_send.at[k], a_recv.at[k], {"x": right}).wait_recv()

    along(None, 0, 0, right)
    along(None, 1, 1, left)
    along(None, 1, 2, right)
    along(None, 0, 3, left)
    own_slot = rows.at[rows_at(tp * ROWS, ROWS)]
    send(lat, own_slot, p_send, p_recv, 0, partner)
    send(wo, wo_mate, m_send, m_recv, 4, partner)

    side = 1 - 2 * c

    def ctx_send(block, k, to):
        slot = cr.at[c, 0, block]
        send(slot, slot, e_send, e_recv, k, {"z": to})

    def ctx_over(block, k):
        send(cr.at[c, 0, block], cr.at[c, 1, block], o_send, o_recv, k, {"y": wrap(y + 2, NY)})

    def ctx_came(block, k):
        slot = cr.at[c, 0, block]
        remote(slot, slot, e_send.at[k], e_recv.at[k], partner).wait_recv()
        send(slot, slot, f_send, f_recv, k, partner)
        ctx_over(block, k)

    def ctx_spread(block, n):
        ctx_send(block, 3 + n, wrap(z + 1, NZ))
        ctx_send(block, 7 + n, wrap(z - 1, NZ))
        ctx_send(block, 11 + n, wrap(z + 2 * side, NZ))

    ctx_send(z, 0, wrap(z + 4, NZ))
    ctx_send(z, 1, wrap(z - 4, NZ))
    ctx_spread(z, 0)
    ctx_over(z, 15)

    for copy in near_copies:
        copy.wait_recv()
    quad = parts[y]
    for k in range(len(near)):
        quad = quad + nbuf[k]
    zsrc[...] = quad

    def z_send_to(src, slot, d):
        return send(src, zbuf.at[slot], z_send, z_recv, slot, {"z": wrap(z + d, NZ)})

    low = z_send_to(zsrc, 0, 4)
    high = z_send_to(zsrc, 1, -4)
    ctx_came(wrap(z - 1, NZ), 3)
    ctx_came(wrap(z + 1, NZ), 7)
    ctx_came(wrap(z - 2 * side, NZ), 11)
    ctx_came(wrap(z - 4, NZ), 0)
    ctx_came(wrap(z + 4, NZ), 1)
    ctx_send(wrap(z - 4 * side, NZ), 2, wrap(z + 4 * side, NZ))
    ctx_spread(wrap(z - 4, NZ), 1)
    ctx_spread(wrap(z + 4, NZ), 2)
    low.wait_recv()
    far = z_send_to(zbuf.at[0], 2, 4)
    high.wait_recv()
    arrived(left, 0, 0)
    along(left, 0, 4, right)
    across_chip(left, 0, 1)
    arrived(right, 1, 1)
    along(right, 1, 5, left)
    across_chip(right, 1, 2)
    ctx_came(wrap(z + 8, NZ), 2)
    ctx_spread(wrap(z + 8, NZ), 3)

    def ctx_group(n):
        step = (0, -4, 4, 8)[n]
        ctx_came(wrap(z - 1 + step, NZ), 3 + n)
        ctx_came(wrap(z + 1 + step, NZ), 7 + n)
        ctx_came(wrap(z - 2 * side + step, NZ), 11 + n)

    ctx_group(1)
    ctx_group(2)
    far.wait_recv()
    total = zsrc[...] + zbuf[0] + zbuf[1] + zbuf[2]
    gsrc[...] = total
    gbuf[tp, y] = total
    g_copies = [
        send(gsrc, gbuf.at[tp, y], g_send, g_recv, k, plane_peer(*p)) for k, p in enumerate(PLANE)
    ]
    arrived(left, 1, 2)
    across_chip(left, 1, 3)
    arrived(right, 0, 3)
    across_chip(right, 0, 4)
    ctx_group(3)
    arrived(across, 0, 4)
    across_chip(across, 0, 5)
    arrived(across, 1, 5)
    across_chip(across, 1, 6)
    for copy in g_copies:
        copy.wait_recv()
    for owner in range(NTP):
        for t in range(2):
            cols = pl.ds((owner * 2 + t) * 128, 128)
            mod[0:4, cols] = gbuf[owner, t]
            mod[4:8, cols] = gbuf[owner, 2 + t]
    tall = (8, WIDTH)
    amp[...] = jnp.broadcast_to(gain[...] * (1.0 + mod[1:2, :]), tall)
    camp[...] = jnp.broadcast_to(gain[...] * (1.0 + mod[5:6, :]), tall)
    shift[...] = jnp.broadcast_to(mod[0:1, :], tall)
    cshift[...] = jnp.broadcast_to(mod[4:5, :], tall)

    for k in range(15):
        slot = cr.at[1 - c, 0, z]
        remote(slot, slot, f_send.at[k], f_recv.at[k], partner).wait_recv()

    def normed(load, store, gains, shifts):
        inverses = []
        for g in range(4):
            acc = jnp.zeros((16, 128), F32)
            for j in range(WIDTH // 128):
                v = load(g, j).astype(F32)
                acc = acc + v * v
            mean = jnp.sum(acc, axis=1, keepdims=True) * (1.0 / WIDTH)
            inverses.append(jnp.broadcast_to(lax.rsqrt(mean + NORM_EPS), (16, 128)))
        for j in range(WIDTH // 128):
            cols = slice(j * 128, j * 128 + 128)
            gain_tile = jnp.concatenate([gains[:, cols]] * 2, axis=0)
            shift_tile = jnp.concatenate([shifts[:, cols]] * 2, axis=0)
            for g in range(4):
                v = load(g, j).astype(F32)
                store(g, cols, (v * inverses[g] * gain_tile + shift_tile).astype(BF16))

    def ctx_project(column):
        def ctx_step(i, carry):
            def load(g, j):
                return cr[j // 8, column, i * 4 + g, :, (j % 8) * 128 : (j % 8) * 128 + 128]

            def store(g, cols, value):
                chid[rows_at((i * 4 + g) * CTX_ROWS, CTX_ROWS), cols] = value

            normed(load, store, camp, cshift)
            return carry

        lax.fori_loop(0, NZ // 4, ctx_step, 0)
        ctxkv[column] = jnp.dot(
            chid[...], wqkv[:, 256:512], preferred_element_type=F32
        ).astype(BF16)

    ctx_project(0)
    ctx_up = send(ctxkv.at[0], ctxkv.at[2], d_send, d_recv, 0, {"y": up})
    ctx_down = send(ctxkv.at[0], ctxkv.at[3], d_send, d_recv, 1, {"y": down})

    remote(lat, rows.at[rows_at((x * NC + 1 - c) * ROWS, ROWS)], p_send.at[0], p_recv.at[0], partner).wait_recv()
    for chip, h, k in [(left, 0, 1), (right, 1, 2), (left, 1, 3), (right, 0, 4), (across, 0, 5), (across, 1, 6)]:
        slot = piece(chip, 1 - c, h)
        remote(slot, slot, p_send.at[k], p_recv.at[k], partner).wait_recv()

    lanes = lax.broadcasted_iota(jnp.int32, (16, 128), 1)
    first = lanes % 64 < 32

    halo = [
        remote(kv.at[pl.ds(GROUP, 128)], kv.at[pl.ds(0, 128)], h_send.at[0], h_recv.at[0], after),
        remote(kv.at[pl.ds(128, 128)], kv.at[pl.ds(GROUP + 128, 128)], h_send.at[1], h_recv.at[1], before),
    ]
    sent.extend(halo)
    for k in range(16):
        slot = cr.at[c, 1, z]
        remote(slot, slot, o_send.at[k], o_recv.at[k], partner).wait_recv()
    send(cr.at[c, 1], cr.at[c, 1], f_send, f_recv, 15, partner)

    def project_step(turn, carry):
        def norm_step(i, carry):
            chip = turn + (i // 3) * (3 - 2 * turn)

            def load(g, j):
                src = rows_at(chip * CHIP + (i % 3) * 64 + g * 16, 16)
                return rows[src, j * 128 : j * 128 + 128]

            def store(g, cols, value):
                hid[rows_at(i * 64 + g * 16, 16), cols] = value

            normed(load, store, amp, shift)
            return carry

        lax.fori_loop(0, 2 * CHIP // 64, norm_step, 0)
        qkv[...] = jnp.dot(hid[...], wqkv[...], preferred_element_type=F32)

        def turn_step(i, carry):
            chip = turn + (i // 6) * (3 - 2 * turn)
            for g in range(2):
                at = rows_at(i * 32 + g * 16, 16)
                start = chip * CHIP + (i % 6) * 32 + g * 16
                to = rows_at(start, 16)
                pad = rows_at(start + WINDOW_REACH, 16)
                cosine, sine = cos_t[to], sin_t[to]
                for h in range(3):
                    u = qkv[at, h * 128 : h * 128 + 128]
                    swapped = jnp.where(first, pltpu.roll(u, 96, 1), pltpu.roll(u, 32, 1))
                    turned = (u * cosine + swapped * sine).astype(BF16)
                    if h < 2:
                        q[to, h * 128 : h * 128 + 128] = turned
                    else:
                        kv[pad, 0:128] = turned
                kv[pad, 128:256] = qkv[at, 384:512].astype(BF16)
            return carry

        lax.fori_loop(0, 2 * CHIP // 32, turn_step, 0)

        @pl.when(turn == 0)
        def _():
            for copy in halo:
                copy.start()

        return carry

    lax.fori_loop(0, 2, project_step, 0)
    whole = cr.at[1 - c, 1]
    remote(whole, whole, f_send.at[15], f_recv.at[15], partner).wait_recv()
    ctx_project(1)
    for copy in halo:
        copy.wait_recv()
    ctx_up.wait_recv()
    ctx_down.wait_recv()

    nt = (((1,), (1,)), ((), ()))
    factor = HEAD_DIM ** (-0.5) * LOG2E
    last = sp * GROUP - WINDOW_REACH

    def attend(chip):
        begin = chip * CHIP
        window = rows_at(begin, WIN)
        key_at = last + begin + lax.broadcasted_iota(jnp.int32, (1, WIN), 1)
        edge = jnp.where((key_at >= 0) & (key_at < GROUP * NZ * NY), 0.0, MASKED_SCORE)
        keys = ctxkv[:, :, 0:128].reshape(1024, 128)
        values = ctxkv[:, :, 128:256].reshape(1024, 128)
        head = lax.broadcasted_iota(jnp.int32, (2 * ROWS, 1), 0)
        sinks = jnp.where(head < ROWS, sink[0:1, 0:1], sink[0:1, 1:2]) * LOG2E

        copy = remote(att.at[chip, 1 - c], att_mate.at[chip], m_send.at[chip], m_recv.at[chip], partner)
        sent.append(copy)

        def part(turn, carry):
            core = lax.rem(1 - c + turn, NC)
            at = rows_at(begin + core * ROWS, ROWS)
            both = jnp.concatenate([q[at, 0:128], q[at, 128:256]], axis=0)
            bias = band[rows_at(core * ROWS, ROWS)] + edge
            near = lax.dot_general(both, kv[window, 0:128], nt, preferred_element_type=F32)
            near = near * factor + jnp.concatenate([bias, bias], axis=0)
            far = lax.dot_general(both, keys, nt, preferred_element_type=F32) * factor
            top = jnp.maximum(
                jnp.maximum(jnp.max(near, axis=1, keepdims=True), jnp.max(far, axis=1, keepdims=True)),
                sinks,
            )
            near = jnp.exp2(near - top)
            far = jnp.exp2(far - top)
            bottom = (
                jnp.sum(near, axis=1, keepdims=True)
                + jnp.sum(far, axis=1, keepdims=True)
                + jnp.exp2(sinks - top)
            )
            mixed = jnp.dot(near.astype(BF16), kv[window, 128:256], preferred_element_type=F32)
            mixed = mixed + jnp.dot(far.astype(BF16), values, preferred_element_type=F32)
            mixed = (mixed / bottom).astype(BF16)
            for h in range(2):
                att[chip, core, :, h * 128 : h * 128 + 128] = mixed[h * ROWS : h * ROWS + ROWS]


            @pl.when(turn == 0)
            def _():
                copy.start()

            return carry

        lax.fori_loop(0, NC, part, 0)
        return copy

    def product(chip, h):
        cols = slice(h * 1024, h * 1024 + 1024)
        return jnp.dot(att[chip, c], wo[:, cols], preferred_element_type=F32) + jnp.dot(
            att_mate[chip], wo_mate[:, cols], preferred_element_type=F32
        )

    def around(src, dst, k, to):
        return send(src, dst, s_send, s_recv, k, {"x": to})

    remote(wo, wo_mate, m_send.at[4], m_recv.at[4], partner).wait_recv()
    attend(across).wait_recv()
    opp_src[0] = product(across, 0).astype(BF16)
    first_left = around(opp_src.at[0], opp_left, 0, right)
    opp_src[1] = product(across, 1).astype(BF16)
    first_right = around(opp_src.at[1], opp_right, 1, left)
    right_mate = attend(right)
    left_mate = attend(left)
    right_mate.wait_recv()
    right_src[1] = product(right, 1).astype(BF16)
    r1 = around(right_src.at[1], from_left.at[1], 2, right)
    left_mate.wait_recv()
    left_src[0] = product(left, 0).astype(BF16)
    l0 = around(left_src.at[0], from_right.at[0], 3, left)
    own_mate = attend(x)
    right_part = product(right, 0)
    first_left.wait_recv()
    right_src[0] = (right_part + opp_left[...].astype(F32)).astype(BF16)
    r0 = around(right_src.at[0], from_left.at[0], 4, right)
    left_part = product(left, 1)
    first_right.wait_recv()
    left_src[1] = (left_part + opp_right[...].astype(F32)).astype(BF16)
    l1 = around(left_src.at[1], from_right.at[1], 5, left)
    own_mate.wait_recv()
    totals = [product(x, h) for h in range(2)]
    for copy in (r1, l0, r0, l1):
        copy.wait_recv()
    for h in range(2):
        cols = slice(h * 1024, h * 1024 + 1024)
        total = totals[h] + from_left[h].astype(F32) + from_right[h].astype(F32)
        out_ref[:, cols] = (lat[:, cols].astype(F32) + mod[2:3, cols] * total).astype(BF16)
    for copy in sent:
        copy.wait_send()


def shards(
    latent,
    condition,
    context_condition,
    context,
    norm_gain,
    shift_weight,
    scale_weight,
    gate_weight,
    query_weight,
    key_matrix,
    value_matrix,
    sink_logit_head,
    out_weight,
):
    lanes = np.arange(HEAD_DIM) % 32
    freq = (10000.0 ** (-(2.0 * lanes) / 64.0)).astype(np.float32)[None]
    vm = pltpu.VMEM
    dma = pltpu.SemaphoreType.DMA
    half = (2, ROWS, WIDTH // 2)
    return pl.pallas_call(
        block_kernel,
        out_shape=jax.ShapeDtypeStruct((ROWS, WIDTH), BF16),
        in_specs=[pl.BlockSpec(memory_space=pl.ANY)] * 14,
        out_specs=pl.BlockSpec(memory_space=pltpu.VMEM),
        scratch_shapes=[
            vm((ROWS, WIDTH), BF16), vm((2, 2, NZ, CTX_ROWS, WIDTH // 2), BF16), vm((1, WIDTH), F32),
            vm((1, 32), F32), vm((1, 32), F32),
            vm((32, 256), BF16), vm((32, 256), BF16), vm((32, 256), BF16),
            vm((WIDTH, 512), BF16), vm((1, 2), F32), vm((256, WIDTH), BF16), vm((1, 128), F32),
            vm((GROUP, WIDTH), BF16),
            vm((4, 4, 128), F32), vm((15, 4, 128), F32), vm((4, 128), F32), vm((3, 4, 128), F32),
            vm((4, 128), F32), vm((NTP, NY, 4, 128), F32),
            vm((8, WIDTH), F32), vm((8, WIDTH), F32), vm((8, WIDTH), F32), vm((8, WIDTH), F32), vm((8, WIDTH), F32),
            vm((GROUP, 128), F32), vm((GROUP, 128), F32), vm((CHIP, WIN), F32),
            vm((2 * CHIP, WIDTH), BF16), vm((NZ * CTX_ROWS, WIDTH), BF16), vm((2 * CHIP, 512), F32),
            vm((GROUP, 256), BF16), vm((GROUP + 256 + 64, 256), BF16),
            vm((NY, NZ * CTX_ROWS, 256), BF16),
            vm((NX, NC, ROWS, 256), BF16), vm((NX, ROWS, 256), BF16), vm((256, WIDTH), BF16),
            vm(half, BF16), vm(half, BF16), vm(half, BF16),
            vm(half[1:], BF16), vm(half[1:], BF16), vm(half, BF16), vm(half, BF16),
            dma((16,)),
            dma((15,)), dma((15,)), dma((3,)), dma((3,)), dma((31,)), dma((31,)),
            dma((6,)), dma((6,)), dma((7,)), dma((7,)),
            dma((15,)), dma((15,)), dma((16,)), dma((16,)), dma((16,)), dma((16,)), dma((2,)), dma((2,)), dma((2,)), dma((2,)),
            dma((5,)), dma((5,)), dma((6,)), dma((6,)),
        ],
        compiler_params=pltpu.CompilerParams(
            collective_id=0, has_side_effects=True, vmem_limit_bytes=62 * 1024 * 1024
        ),
        cost_estimate=pl.CostEstimate(flops=10**9, bytes_accessed=10**7, transcendentals=0),
        name="block",
    )(
        latent, context, norm_gain.reshape(1, -1), condition.reshape(1, -1),
        context_condition.reshape(1, -1), shift_weight, scale_weight, gate_weight,
        query_weight, key_matrix, value_matrix, sink_logit_head.reshape(1, -1), out_weight,
        jnp.asarray(freq),
    )


def solution(mesh):
    torus = Mesh(mesh.devices.reshape(NZ, NY, NX, NC), ALL)
    return jax.shard_map(
        shards,
        mesh=torus,
        in_specs=(
            P(ALL, None),
            P(SP),
            P(SP),
            P(SP, None),
            P(),
            P(SP, TP),
            P(SP, TP),
            P(SP, TP),
            P(None, TP),
            P(None, TP),
            P(None, TP),
            P(TP),
            P(TP, None),
        ),
        out_specs=P(ALL, None),
        check_vma=False,
    )
```
